32 devices in a mesh: rep: 2 (over x), fs: 8 (over z, y), tp: 2 (over core).
Axes of the slice: x: 2, y: 2, z: 4, core: 2. Of those that a mesh axis runs over, the one named last changes fastest.
Arguments:
- tokens: bfloat16 [16, 64, 2048], P(('rep', 'fs'), None, 'tp'), may hold values from -6 to 6
- lin_weight: bfloat16 [2048, 1024], P('fs', 'tp'), may hold values from -0.125 to 0.125
- glu_weight: bfloat16 [2048, 1024], P('fs', 'tp'), may hold values from -0.125 to 0.125
- conv_taps: float32 [31, 1024], P(None, 'tp'), may hold values from -4 to 4
- conv_gain: float32 [1024], P('tp'), may hold values from 0.1 to 1.9
- conv_out_weight: bfloat16 [1024, 2048], P('tp', 'fs'), may hold values from -0.1875 to 0.1875
- mix_gain: float32 [2048], replicated, may hold values from 0.1 to 1.9
- ff_gate: bfloat16 [2048, 5632], P('fs', 'tp'), may hold values from -0.125 to 0.125
- ff_up: bfloat16 [2048, 5632], P('fs', 'tp'), may hold values from -0.125 to 0.125
- ff_down: bfloat16 [5632, 2048], P('tp', 'fs'), may hold values from -0.078125 to 0.078125
- out_gain: float32 [2048], replicated, may hold values from 0.1 to 1.9
Outputs:
- encoded: bfloat16 [16, 64, 2048], P(('rep', 'fs'), None, 'tp')
The draws below stay inside these ranges and needn't reach their ends.
All inputs are finite; a program needn't handle non-finite values.
Results may differ from the reference program's by a relative error of at most 0.014.
Values may be sent and summed in bfloat16 or wider, within the bound.
A program may use at most 128 MiB of HBM per device.

```python
import jax
import jax.numpy as jnp
from jax import lax

D = 2048
CONV = 1024
FF = 5632
TAPS = 31
TOK_DEV = 64
SEQUENCES = 16
N_TP = 2


def draw_conv_taps(key, part):
    first, second = jax.random.split(jax.random.fold_in(key, 17))
    channel = jnp.arange(CONV, dtype=jnp.float32)
    ramp = 3.0 ** (2.0 * channel / CONV - 1.0)
    spread = jnp.exp(jax.random.uniform(second, (CONV,), jnp.float32, -0.5, 0.5))
    base = jnp.clip(jax.random.normal(first, (TAPS, CONV), jnp.float32), -4.0, 4.0)
    return (base * TAPS ** (-0.5) * ramp * spread).astype(jnp.float32)


def shard_levels(key, shape, cuts, smallest, largest):
    def one(dim, parts):
        steps = jax.random.uniform(jax.random.fold_in(jax.random.fold_in(key, 6), dim), (parts,), jnp.float32, smallest / len(cuts), largest / len(cuts))
        return jnp.repeat(jnp.exp(steps), shape[dim] // parts).reshape((-1,) + (1,) * (len(shape) - dim - 1))

    factor_of = one(*cuts[0])
    for cut in cuts[1:]:
        factor_of = factor_of * one(*cut)
    return factor_of


def bell_draw(own_key, dims, deviation, bound, pieces=(), kind=jnp.bfloat16):
    values = deviation * jax.random.normal(own_key, dims, jnp.float32)
    if pieces:
        values = values * shard_levels(own_key, dims, pieces, -0.22, 0.18)
    return jnp.clip(values, -bound, bound).astype(kind)


def setup_inputs(seed: int = 0) -> dict:
    keys = jax.random.split(jax.random.key(seed), 12)
    return {
        "tokens": bell_draw(keys[0], (SEQUENCES, TOK_DEV, D), 1.0, 6.0, ((0, 16), (2, 2))),
        "lin_weight": bell_draw(keys[1], (D, CONV), D ** -0.5, 0.125, ((0, 8), (1, 2))),
        "glu_weight": bell_draw(keys[2], (D, CONV), D ** -0.5, 0.125, ((0, 8), (1, 2))),
        "conv_taps": draw_conv_taps(jax.random.fold_in(keys[11], 71), 0),
        "conv_gain": jnp.clip(1.0 + 0.18 * jax.random.normal(keys[4], (CONV,), jnp.float32), 0.1, 1.9),
        "conv_out_weight": bell_draw(keys[5], (CONV, D), CONV ** -0.5, 0.1875, ((0, 2), (1, 8))),
        "mix_gain": jnp.clip(1.0 + 0.18 * jax.random.normal(keys[6], (D,), jnp.float32), 0.1, 1.9),
        "ff_gate": bell_draw(keys[7], (D, FF), D ** -0.5, 0.125, ((0, 8), (1, 2))),
        "ff_up": bell_draw(keys[8], (D, FF), D ** -0.5, 0.125, ((0, 8), (1, 2))),
        "ff_down": bell_draw(keys[9], (FF, D), FF ** -0.5, 0.078125, ((0, 2), (1, 8))),
        "out_gain": jnp.clip(1.0 + 0.18 * jax.random.normal(keys[10], (D,), jnp.float32), 0.1, 1.9),
    }


residual_scale = 2.0 ** 0.25
epsilon = 1e-05

def rounded(value):
    return lax.optimization_barrier(value.astype(jnp.bfloat16)).astype(jnp.float32)

def normalize(values):
    average = lax.optimization_barrier(jnp.mean(values, axis=-1, keepdims=True))
    squares = lax.optimization_barrier(jnp.mean(values * values, axis=-1, keepdims=True))
    return (values - average) * lax.rsqrt(squares - average * average + epsilon)

def block_sum(left, right):
    rows, inner = left.shape
    width = inner // N_TP
    left_blocks = left.astype(jnp.float32).reshape(rows, N_TP, width)
    right_blocks = right.astype(jnp.float32).reshape(N_TP, width, right.shape[1])
    partial_value = jnp.einsum('tjc,jcd->jtd', left_blocks, right_blocks)
    return lax.optimization_barrier(jnp.sum(rounded(partial_value), axis=0))

def depthwise(values, conv_taps):
    margin = (TAPS - 1) // 2
    return lax.conv_general_dilated(values[None], conv_taps[:, None, :], (1,), [(margin, margin)], dimension_numbers=('NWC', 'WIO', 'NWC'), feature_group_count=values.shape[1], precision=lax.Precision.HIGHEST)[0]

def reference(tokens, lin_weight, glu_weight, conv_taps, conv_gain, conv_out_weight, mix_gain, ff_gate, ff_up, ff_down, out_gain):

    def one_sequence(inputs):
        linear = jnp.dot(inputs, lin_weight, preferred_element_type=jnp.float32)
        gating = jnp.dot(inputs, glu_weight, preferred_element_type=jnp.float32)
        glu = (linear * jax.nn.sigmoid(gating)).astype(jnp.bfloat16)
        conv = depthwise(glu.astype(jnp.float32), conv_taps)
        activated = jax.nn.silu(normalize(conv) * conv_gain).astype(jnp.bfloat16)
        mixed = rounded(block_sum(activated, conv_out_weight))
        middle = (normalize(residual_scale * inputs.astype(jnp.float32) + mixed) * mix_gain).astype(jnp.bfloat16)
        gate = jnp.dot(middle, ff_gate, preferred_element_type=jnp.float32)
        upward = jnp.dot(middle, ff_up, preferred_element_type=jnp.float32)
        hidden = (jax.nn.silu(gate) * upward).astype(jnp.bfloat16)
        forward = rounded(block_sum(hidden, ff_down))
        total = residual_scale * middle.astype(jnp.float32) + forward
        return (normalize(total) * out_gain).astype(jnp.bfloat16)
    return lax.map(one_sequence, tokens)
```

```python
import functools

import jax
import jax.numpy as jnp
from jax import lax
from jax.experimental import pallas as pl
from jax.experimental.pallas import tpu as pltpu
from jax.sharding import PartitionSpec as P

residual_scale = 2.0**0.25
epsilon = 1e-05


def normed(values):
    average = jnp.mean(values, axis=-1, keepdims=True)
    second = jnp.mean(values * values, axis=-1, keepdims=True)
    return (values - average) * lax.rsqrt(second - average * average + epsilon)


def interleave(left, right, parts):
    rows, width = left.shape
    pair = jnp.concatenate(
        (left.reshape(rows, parts, width // parts), right.reshape(rows, parts, width // parts)),
        axis=2,
    )
    return pair.reshape(rows, 2 * width)


def by_collectives(
    tokens,
    lin_weight,
    glu_weight,
    conv_taps,
    conv_gain,
    conv_out_weight,
    mix_gain,
    ff_gate,
    ff_up,
    ff_down,
    out_gain,
):
    n_fs, n_tp = lax.axis_size("fs"), lax.axis_size("tp")
    fs_index, tp_index = lax.axis_index("fs"), lax.axis_index("tp")
    seqs, length, feat = tokens.shape
    groups = n_fs * seqs
    rows = groups * length
    model = feat * n_tp
    conv_gain_all = lax.all_gather(conv_gain, "tp", axis=0, tiled=True)

    gathered = lax.all_gather(tokens, ("fs", "tp"), axis=0, tiled=False)
    all_tokens = (
        gathered.reshape(n_fs, n_tp, seqs, length, feat)
        .transpose(0, 2, 3, 1, 4)
        .reshape(rows, model)
    )
    glu_pair = lax.all_to_all(
        interleave(lin_weight, glu_weight, n_fs), "fs", split_axis=1, concat_axis=0, tiled=True
    )
    own_out = lax.all_to_all(conv_out_weight, "tp", split_axis=1, concat_axis=0, tiled=True)
    ff_pair = lax.all_to_all(
        interleave(ff_gate, ff_up, n_fs), "fs", split_axis=1, concat_axis=0, tiled=True
    )
    own_down = lax.all_to_all(ff_down, "fs", split_axis=0, concat_axis=1, tiled=True)

    chans = glu_pair.shape[1] // 2
    product = jnp.dot(all_tokens, glu_pair, preferred_element_type=jnp.float32)
    glu = (product[:, :chans] * jax.nn.sigmoid(product[:, chans:])).astype(jnp.bfloat16)
    n_taps = conv_taps.shape[0]
    margin = (n_taps - 1) // 2
    own_taps = lax.dynamic_slice_in_dim(conv_taps, fs_index * chans, chans, 1)
    padded = jnp.pad(
        glu.astype(jnp.float32).reshape(groups, length, chans),
        ((0, 0), (margin, margin), (0, 0)),
    )
    conv = sum(padded[:, k : k + length] * own_taps[k] for k in range(n_taps))
    conv = conv.reshape(rows, chans).astype(jnp.bfloat16)
    conv_all = lax.all_gather(conv, ("tp", "fs"), axis=1, tiled=True)
    activated = jax.nn.silu(normed(conv_all.astype(jnp.float32)) * conv_gain_all).astype(
        jnp.bfloat16
    )
    mixed_own = jnp.dot(activated, own_out, preferred_element_type=jnp.float32).astype(
        jnp.bfloat16
    )
    mixed = lax.all_gather(mixed_own, ("fs", "tp"), axis=1, tiled=True)
    before = residual_scale * all_tokens.astype(jnp.float32) + mixed.astype(jnp.float32)
    middle = (normed(before) * mix_gain).astype(jnp.bfloat16)

    units = ff_pair.shape[1] // 2
    both = jnp.dot(middle, ff_pair, preferred_element_type=jnp.float32)
    hidden = (jax.nn.silu(both[:, :units]) * both[:, units:]).astype(jnp.bfloat16)
    down = jnp.dot(hidden, own_down, preferred_element_type=jnp.float32).astype(jnp.bfloat16)
    sends = (
        down.reshape(n_fs, seqs * length, n_tp, feat)
        .transpose(0, 2, 1, 3)
        .reshape(n_fs * n_tp, seqs * length, feat)
    )
    arrived = lax.all_to_all(sends, ("fs", "tp"), split_axis=0, concat_axis=0, tiled=True)
    forward = jnp.sum(arrived.astype(jnp.float32), axis=0)
    forward = forward.astype(jnp.bfloat16).astype(jnp.float32)
    middle_own = lax.dynamic_slice(
        middle,
        (fs_index * seqs * length, tp_index * feat),
        (seqs * length, feat),
    )
    final = residual_scale * middle_own.astype(jnp.float32) + forward
    sums, squares = lax.psum(
        (jnp.sum(final, axis=1, keepdims=True), jnp.sum(final * final, axis=1, keepdims=True)),
        "tp",
    )
    average = sums / model
    out = (final - average) * lax.rsqrt(squares / model - average * average + epsilon)
    gain = lax.dynamic_slice_in_dim(out_gain, tp_index * feat, feat, 0)
    return (out * gain).astype(jnp.bfloat16).reshape(seqs, length, feat)


MESH = pl.DeviceIdType.MESH
LANES = 128
FIRST = ((2, 0), (3, 0))
CROSS = ((2, 1), (3, 1))
NEAR = ((1, 0), (1, 1), (0, 1))
OTHERS = FIRST + CROSS + NEAR
G, U, D = 0, 1, 2
SENDS = {
    "t0": ((G, 2, 0),),
    "t3": ((U, 2, 0),),
    "t5": ((G, 3, 0), (G, 1, 0), (U, 3, 0)),
    "t7": ((G, 0, 1),),
    "c0": ((G, 2, 1),),
    "c5": ((U, 2, 1), (U, 1, 0)),
    "c7": ((G, 3, 1), (U, 0, 1), (G, 1, 1)),
    "m0": ((U, 3, 1),),
    "m3": ((U, 1, 1), (D, 2, 0)),
    "m5": ((D, 3, 0),),
    "m7": ((D, 2, 1), (D, 3, 1), (D, 1, 0), (D, 1, 1), (D, 0, 1)),
}
FORWARDS = {
    "c0": ((G, 2, 0), (U, 2, 0)),
    "c4": ((G, 3, 0),),
    "c6": ((G, 1, 0), (U, 3, 0), (G, 0, 1)),
    "m0": ((G, 2, 1),),
    "m2": ((U, 2, 1), (U, 1, 0)),
    "m4": ((G, 3, 1), (U, 0, 1)),
    "m6": ((G, 1, 1), (U, 3, 1)),
    "m8": ((U, 1, 1), (D, 2, 0)),
    "f0": ((D, 3, 0),),
    "f1": ((D, 2, 1), (D, 3, 1), (D, 1, 0), (D, 1, 1), (D, 0, 1)),
}

def fused(
    n_fs,
    n_tp,
    width,
    narrow,
    tok,
    lin_hbm,
    glu_hbm,
    taps_hbm,
    gain,
    out_weight,
    mix_gain,
    gate_hbm,
    up_hbm,
    down_hbm,
    out_gain,
    out,
    x_s,
    lin_s,
    gl_s,
    taps_s,
    mix_s,
    glu_s,
    gain_s,
    proj_s,
    pad_s,
    conv_s,
    norm_s,
    act_s,
    mixed_s,
    mid_s,
    gate_s,
    up_s,
    down_s,
    hid_s,
    part_s,
    half_s,
    sum_s,
    q_s,
    y_s,
    stat_s,
    glu_sems,
    glu_cross_sems,
    small_sems,
    tok_sems,
    conv_sems,
    mixed_sems,
    ff_sems,
    cross_sems,
    local_sems,
    half_sems,
    q_sems,
    y_sems,
):
    rep, f, t = lax.axis_index("rep"), lax.axis_index("fs"), lax.axis_index("tp")
    other = 1 - t
    n_hi = n_fs // 2
    hi, lo = f // 2, f % 2
    rows, feat = x_s.shape[1:]
    length = rows // n_fs
    model = feat * n_tp
    depth = gate_hbm.shape[0]
    half_depth = depth // 2
    chans = LANES // 2
    pending = []

    def flip(z, step):
        return z + step - 2 * step * ((z // step) % 2)

    def along(k):
        z = hi
        for step in (1, 2):
            if k[0] & step:
                z = flip(z, step)
        return z * 2 + (1 - lo if k[1] else lo)

    def code(k):
        return k[0] * 2 + k[1]

    barrier = pltpu.get_barrier_semaphore()
    for k in OTHERS:
        pl.semaphore_signal(barrier, inc=1, device_id=(rep, along(k), t), device_id_type=MESH)
    pl.semaphore_signal(barrier, inc=1, device_id=(rep, f, other), device_id_type=MESH)
    pl.semaphore_signal(barrier, inc=1, device_id=(1 - rep, f, t), device_id_type=MESH)

    def rows_of(i):
        return pl.ds(pl.multiple_of(i * length, length), length)

    def depth_of(i, part, size):
        return pl.ds(pl.multiple_of(i * depth + part * half_depth, half_depth), size)

    def tok_slot(i, j):
        return x_s.at[j, rows_of(i)]

    per_half = n_fs // 2

    def start_of(i):
        return pl.multiple_of((i * (width // LANES) - i // per_half) * LANES, LANES)

    def is_short(i):
        return i % per_half == per_half - 1

    def sized(i, action):
        @pl.when(jnp.logical_not(is_short(i)))
        def _():
            action(width)

        @pl.when(is_short(i))
        def _():
            action(narrow)

    fetches = [
        pltpu.make_async_copy(src, dst, local_sems.at[n])
        for n, (src, dst) in enumerate(
            (
                (tok, tok_slot(f, t)),
                (lin_hbm, lin_s),
                (glu_hbm, gl_s),
                (taps_hbm, taps_s),
            )
        )
    ]
    for copy in fetches:
        copy.start()

    def own_copy(which, size):
        first = start_of(f)
        src, dst = (
            (gate_hbm.at[:, pl.ds(first, size)], gate_s.at[depth_of(f, 0, depth), pl.ds(0, size)]),
            (up_hbm.at[:, pl.ds(first, size)], up_s.at[depth_of(f, 0, depth), pl.ds(0, size)]),
            (down_hbm.at[pl.ds(first, size)], down_s.at[f, pl.ds(0, size)]),
        )[which]
        return pltpu.make_async_copy(src, dst, local_sems.at[4 + which])

    for which in range(3):
        sized(f, lambda size, which=which: own_copy(which, size).start())

    @pl.when(is_short(f))
    def _():
        gate_s[:, narrow:] = jnp.zeros((n_fs * depth, width - narrow), jnp.bfloat16)
        up_s[:, narrow:] = jnp.zeros((n_fs * depth, width - narrow), jnp.bfloat16)
        down_s[:, narrow:, :] = jnp.zeros((n_fs, width - narrow, down_s.shape[2]), jnp.bfloat16)

    def remote(src, dst, sems, index, device):
        return pltpu.make_async_remote_copy(
            src_ref=src,
            dst_ref=dst,
            send_sem=sems.at[0, index],
            recv_sem=sems.at[1, index],
            device_id=device,
            device_id_type=MESH,
        )

    def send(*parts):
        copy = remote(*parts)
        copy.start()
        pending.append(copy.wait_send)

    partner = (rep, f, other)
    mirror = (1 - rep, f, t)
    beside = (rep, along((0, 1)), t)
    close = (rep, along((1, 0)), t)
    far = (rep, along((2, 0)), t)

    def receive(dst, sems, index):
        remote(dst, dst, sems, index, partner).wait_recv()

    def gather_start(slot, sems):
        block = slot(f, t)
        send(block, block, sems, 0, far)
        send(block, block, sems, 1, close)
        send(block, block, sems, 3, beside)
        send(block, block, sems, 7, partner)

    def slot(name):
        for which, *k in SENDS.get(name, ()):
            weight_send(which, tuple(k))
        for which, *k in FORWARDS.get(name, ()):
            weight_forward(which, tuple(k))

    def gather_finish(place, sems, name, between=None):
        between = between or {}

        def pause(step):
            slot(name + str(step))
            if step in between:
                between[step]()

        def got(index, k):
            block = place(along(k), t)
            receive(block, sems, index)
            return block

        block = got(1, (1, 0))
        send(block, block, sems, 4, beside)
        send(block, block, sems, 7 + code((1, 0)), partner)
        pause(1)
        block = got(3, (0, 1))
        send(block, block, sems, 7 + code((0, 1)), partner)
        pause(2)
        block = got(0, (2, 0))
        send(block, block, sems, 2, close)
        send(block, block, sems, 5, beside)
        send(block, block, sems, 7 + code((2, 0)), partner)
        pause(3)
        block = got(4, (1, 1))
        send(block, block, sems, 7 + code((1, 1)), partner)
        pause(4)
        block = got(2, (3, 0))
        send(block, block, sems, 6, beside)
        send(block, block, sems, 7 + code((3, 0)), partner)
        pause(5)
        block = got(5, (2, 1))
        send(block, block, sems, 7 + code((2, 1)), partner)
        pause(6)
        block = got(6, (3, 1))
        send(block, block, sems, 7 + code((3, 1)), partner)
        pause(7)
        for k in ((0, 0),) + OTHERS:
            receive(place(along(k), other), sems, 7 + code(k))

    half_width = width // 2

    def piece(which, to, source, part, size):
        first = start_of(to)
        ups = pl.ds(pl.multiple_of(part * half_depth, half_depth), half_depth)
        spot = depth_of(source, part, half_depth)
        deep = pl.ds(pl.multiple_of(part * (size // 2), size // 2), size // 2)
        from_down = pl.ds(pl.multiple_of(first + part * (size // 2), LANES // 2), size // 2)
        return (
            (gate_hbm.at[ups, pl.ds(first, size)], gate_s.at[spot, pl.ds(0, size)]),
            (up_hbm.at[ups, pl.ds(first, size)], up_s.at[spot, pl.ds(0, size)]),
            (down_hbm.at[from_down], down_s.at[source, deep]),
        )[which]

    def weight_send(which, k):
        to = along(k)

        def copy(size):
            src, dst = piece(which, to, f, rep, size)
            return remote(src, dst, ff_sems, which * n_fs + code(k), (rep, to, t))

        sized(to, lambda size: copy(size).start())
        pending.append(lambda: sized(to, lambda size: copy(size).wait_send()))

    def weight_forward(which, k):
        index = which * n_fs + code(k)

        def block(size):
            return piece(which, f, along(k), rep, size)[1]

        def action(size):
            receive(block(size), ff_sems, index)
            remote(block(size), block(size), cross_sems, index, mirror).start()

        sized(f, action)
        pending.append(
            lambda: sized(
                f,
                lambda size: remote(
                    block(size), block(size), cross_sems, index, mirror
                ).wait_send(),
            )
        )

    def weight_finish(which):
        for k in OTHERS:
            sized(
                f,
                lambda size: receive(
                    piece(which, f, along(k), 1 - rep, size)[1], cross_sems, which * n_fs + code(k)
                ),
            )

    pl.semaphore_wait(barrier, n_fs + 1)
    fetches[0].wait()
    gather_start(tok_slot, tok_sems)
    fetches[1].wait()
    fetches[2].wait()
    for d in range(n_fs):
        cols = slice(d * chans, (d + 1) * chans)
        mix_s[d] = jnp.concatenate((lin_s[:, cols], gl_s[:, cols]), axis=1)

    def glu_piece(source, part):
        return glu_s.at[depth_of(source, part, half_depth)]

    for k in OTHERS:
        to = along(k)
        own_rows = pl.ds(pl.multiple_of(rep * half_depth, half_depth), half_depth)
        send(mix_s.at[to, own_rows], glu_piece(f, rep), glu_sems, code(k), (rep, to, t))
    slot("t0")
    columns = pl.ds(pl.multiple_of(other * LANES, LANES), LANES)
    own_columns = pl.ds(pl.multiple_of(t * LANES, LANES), LANES)
    send(gain, gain_s.at[t], small_sems, 0, partner)
    send(out_weight.at[:, columns], proj_s.at[t], small_sems, 1, partner)

    glu_s[pl.ds(pl.multiple_of(f * depth, depth), depth), :] = mix_s[f]
    gain_s[t] = gain[...]
    proj_s[t] = out_weight[:, own_columns]
    pad_s[...] = jnp.zeros_like(pad_s)

    def glu_forward(ks):
        for k in ks:
            block = glu_piece(along(k), rep)
            receive(block, glu_sems, code(k))
            send(block, block, glu_cross_sems, code(k), mirror)

    gather_finish(
        tok_slot,
        tok_sems,
        "t",
        {
            4: lambda: glu_forward(NEAR),
            5: lambda: glu_forward(FIRST),
            6: lambda: glu_forward(CROSS),
        },
    )
    for k in OTHERS:
        receive(glu_piece(along(k), 1 - rep), glu_cross_sems, code(k))

    product = sum(
        jnp.dot(
            x_s[j], glu_s[j * feat : (j + 1) * feat], preferred_element_type=jnp.float32
        )
        for j in range(n_tp)
    )
    glu = product[:, :chans] / (1.0 + jnp.exp(-product[:, chans:]))
    top = rows // 2
    packed = jnp.concatenate((glu[:top], glu[top:]), axis=1)
    packed = packed.astype(jnp.bfloat16).astype(jnp.float32)
    fetches[3].wait()
    lanes = lax.broadcasted_iota(jnp.int32, (1, LANES), 1)
    tap_pair = taps_s[:, pl.ds(pl.multiple_of(f // 2 * LANES, LANES), LANES)]
    turned = pltpu.roll(tap_pair, chans, 1)
    taps = jnp.where((lanes < chans) == (f % 2 == 0), tap_pair, turned)
    n_taps = taps.shape[0]
    margin = (n_taps - 1) // 2
    conv_slot = lambda i, j: conv_s.at[j * n_fs + i]
    groups = n_fs // 2
    for g in range(groups):
        pad_s[g, 16 : 16 + length, :] = packed[g * length : (g + 1) * length]
    for g in range(groups):
        acc = jnp.zeros((length, LANES), jnp.float32)
        for k in range(n_taps):
            first = 16 - margin + k
            acc = acc + pad_s[g, first : first + length, :] * taps[k : k + 1, :]
        conv_s[t * n_fs + f, g * length : (g + 1) * length, :] = acc.astype(jnp.bfloat16)
    gather_start(conv_slot, conv_sems)
    slot("c0")
    gather_finish(conv_slot, conv_sems, "c")
    receive(gain_s.at[other], small_sems, 0)
    receive(proj_s.at[other], small_sems, 1)

    for j in range(n_fs * n_tp // 2):
        left = conv_s[2 * j].astype(jnp.float32)
        right = conv_s[2 * j + 1].astype(jnp.float32)
        cols = slice(j * LANES, (j + 1) * LANES)
        norm_s[:top, cols] = jnp.concatenate((left[:, :chans], right[:, :chans]), axis=1)
        norm_s[top:, cols] = jnp.concatenate((left[:, chans:], right[:, chans:]), axis=1)
    gains = jnp.concatenate([gain_s[j] for j in range(n_tp)], axis=1)

    @pl.loop(0, n_fs)
    def _(i):
        here = rows_of(i)
        v = normed(norm_s[here, :]) * gains
        act_s[here, :] = (v / (1.0 + jnp.exp(-v))).astype(jnp.bfloat16)

    share = proj_s.shape[1]
    mixed_slot = lambda i, j: mixed_s.at[i * n_tp + j]
    mixed_s[f * n_tp + t] = sum(
        jnp.dot(
            act_s[:, j * share : (j + 1) * share],
            proj_s[j],
            preferred_element_type=jnp.float32,
        )
        for j in range(n_tp)
    ).astype(jnp.bfloat16)
    gather_start(mixed_slot, mixed_sems)
    slot("m0")
    gather_finish(mixed_slot, mixed_sems, "m")
    slot("m8")

    @pl.loop(0, n_fs)
    def _(i):
        here = rows_of(i)
        skip = jnp.concatenate([x_s[j, here, :] for j in range(n_tp)], axis=1)
        added = jnp.concatenate([mixed_s[j, here, :] for j in range(n_fs * n_tp)], axis=1)
        before = residual_scale * skip.astype(jnp.float32) + added.astype(jnp.float32)
        mid_s[here, :] = (normed(before) * mix_gain[...]).astype(jnp.bfloat16)

    slot("f0")
    for which in range(3):
        sized(f, lambda size, which=which: own_copy(which, size).wait())
    weight_finish(0)
    weight_finish(1)

    for i in range(2):
        here = pl.ds(i * top, top)
        gate = jnp.dot(mid_s[here, :], gate_s[...], preferred_element_type=jnp.float32)
        upward = jnp.dot(mid_s[here, :], up_s[...], preferred_element_type=jnp.float32)
        value = gate / (1.0 + jnp.exp(-gate)) * upward
        hid_s[here, :] = value.astype(jnp.bfloat16)
        if i == 0:
            slot("f1")

    weight_finish(2)
    span = down_s.shape[2]
    per_core = n_fs // n_tp

    def project(side):
        @pl.loop(0, per_core)
        def _(j):
            part_s[side, :, pl.ds(pl.multiple_of(j * span, span), span)] = jnp.dot(
                hid_s[...], down_s[side * per_core + j], preferred_element_type=jnp.float32
            ).astype(jnp.bfloat16)

    def toward(step, low):
        return ((hi + step) % n_hi) * 2 + low

    steps = list(range(1, n_hi)) + [0]
    project(other)
    for d in steps:
        for e, low in enumerate((1 - lo, lo)):
            here = rows_of(toward(d, low))
            send(part_s.at[other, here], half_s.at[here], half_sems, 2 * d + e, partner)
    project(t)
    for d in steps:
        here = rows_of(toward(d, 1 - lo))
        receive(half_s.at[here], half_sems, 2 * d)
        both = part_s[t, here, :].astype(jnp.float32) + half_s[here, :].astype(jnp.float32)
        sum_s[here, :] = both.astype(jnp.bfloat16)
        send(sum_s.at[here], y_s.at[d], y_sems, d, (rep, hi * 2 + 1 - lo, t))
    for d in steps:
        to = toward(d, lo)
        here = rows_of(to)
        receive(half_s.at[here], half_sems, 2 * d + 1)
        both = part_s[t, here, :].astype(jnp.float32) + half_s[here, :].astype(jnp.float32)
        receive(y_s.at[d], y_sems, d)
        forward = both + y_s[d].astype(jnp.float32)
        if d:
            sum_s[here, :] = forward.astype(jnp.bfloat16)
            send(sum_s.at[here], q_s.at[d], q_sems, d, (rep, to, t))
    for d in range(1, n_hi):
        receive(q_s.at[d], q_sems, d)
        forward = forward + q_s[d].astype(jnp.float32)
    forward = forward.astype(jnp.bfloat16).astype(jnp.float32)
    own_half = pl.ds(pl.multiple_of(t * feat, feat), feat)
    final = residual_scale * mid_s[rows_of(f), own_half].astype(jnp.float32) + forward
    lane = lax.broadcasted_iota(jnp.int32, (length, LANES), 1)
    stat_s[t] = jnp.where(
        lane == 0,
        jnp.sum(final, axis=1, keepdims=True),
        jnp.sum(final * final, axis=1, keepdims=True),
    )
    send(stat_s.at[t], stat_s.at[t], small_sems, 2, partner)
    receive(stat_s.at[other], small_sems, 2)
    stats = (stat_s[0] + stat_s[1]) / model
    average, second = stats[:, 0:1], stats[:, 1:2]
    scaled = (final - average) * lax.rsqrt(second - average * average + epsilon)
    out[...] = (scaled * out_gain[t]).astype(jnp.bfloat16)
    for wait in pending:
        wait()


def by_kernel(
    tokens,
    lin_weight,
    glu_weight,
    conv_taps,
    conv_gain,
    conv_out_weight,
    mix_gain,
    ff_gate,
    ff_up,
    ff_down,
    out_gain,
):
    n_fs, n_tp = lax.axis_size("fs"), lax.axis_size("tp")
    _, length, feat = tokens.shape
    rows, model = n_fs * length, feat * n_tp
    depth, own_chans = lin_weight.shape
    chans = own_chans // n_fs
    width, narrow = widths(ff_gate.shape[1], n_fs)
    vmem, far = pl.BlockSpec(memory_space=pltpu.VMEM), pl.BlockSpec(memory_space=pl.ANY)
    bf, fl = jnp.bfloat16, jnp.float32
    span = ff_down.shape[1]
    pair = lambda n: pltpu.SemaphoreType.DMA((2, n))
    result = pl.pallas_call(
        functools.partial(fused, n_fs, n_tp, width, narrow),
        out_shape=jax.ShapeDtypeStruct((length, feat), bf),
        in_specs=[far] * 4 + [vmem] * 3 + [far] * 3 + [vmem],
        out_specs=vmem,
        scratch_shapes=[
            pltpu.VMEM((n_tp, rows, feat), bf),
            pltpu.VMEM((depth, own_chans), bf),
            pltpu.VMEM((depth, own_chans), bf),
            pltpu.VMEM(conv_taps.shape, fl),
            pltpu.VMEM((n_fs, depth, 2 * chans), bf),
            pltpu.VMEM((n_fs * depth, 2 * chans), bf),
            pltpu.VMEM((n_tp, 1, own_chans), fl),
            pltpu.VMEM((n_tp, own_chans, span // n_tp), bf),
            pltpu.VMEM((n_fs // 2, length + 32, LANES), fl),
            pltpu.VMEM((n_fs * n_tp, rows // 2, LANES), bf),
            pltpu.VMEM((rows, own_chans * n_tp), fl),
            pltpu.VMEM((rows, own_chans * n_tp), bf),
            pltpu.VMEM((n_fs * n_tp, rows, LANES), bf),
            pltpu.VMEM((rows, model), bf),
            pltpu.VMEM((n_fs * depth, width), bf),
            pltpu.VMEM((n_fs * depth, width), bf),
            pltpu.VMEM((n_fs, width, span), bf),
            pltpu.VMEM((rows, width), bf),
            pltpu.VMEM((n_tp, rows, feat), bf),
            pltpu.VMEM((rows, feat), bf),
            pltpu.VMEM((rows, feat), bf),
            pltpu.VMEM((n_fs // 2, length, feat), bf),
            pltpu.VMEM((n_fs // 2, length, feat), bf),
            pltpu.VMEM((n_tp, length, LANES), fl),
            pair(n_fs),
            pair(n_fs),
            pair(3),
            pair(2 * n_fs),
            pair(2 * n_fs),
            pair(2 * n_fs),
            pair(3 * n_fs),
            pair(3 * n_fs),
            pltpu.SemaphoreType.DMA((7,)),
            pair(n_fs),
            pair(n_fs // 2),
            pair(n_fs // 2),
        ],
        compiler_params=pltpu.CompilerParams(
            collective_id=0, has_side_effects=True, vmem_limit_bytes=60 * 2**20
        ),
    )(
        tokens[0],
        lin_weight,
        glu_weight,
        conv_taps,
        conv_gain[None],
        conv_out_weight,
        mix_gain[None],
        ff_gate,
        ff_up,
        ff_down,
        out_gain.reshape(n_tp, 1, feat),
    )
    return result[None]


def widths(units, n_fs):
    half = n_fs // 2
    blocks = units // LANES // 2
    most = -(-blocks // half)
    return most * LANES, (blocks - most * (half - 1)) * LANES


def on_device(*args):
    tokens, lin_weight, conv_out_weight, ff_gate = args[0], args[1], args[5], args[7]
    n_fs, n_tp, n_rep = (lax.axis_size(a) for a in ("fs", "tp", "rep"))
    seqs, length, feat = tokens.shape
    units = ff_gate.shape[1]
    width, narrow = widths(units, n_fs)
    fits = (
        n_rep == 2
        and n_tp == 2
        and n_fs == 8
        and seqs == 1
        and length % 16 == 0
        and args[3].shape[0] <= 33
        and lin_weight.shape[1] * 2 == n_fs * LANES
        and conv_out_weight.shape[1] == n_tp * LANES
        and feat % LANES == 0
        and units % (2 * LANES) == 0
        and narrow == width - LANES > 0
        and lin_weight.shape[0] % 32 == 0
    )
    if fits:
        return by_kernel(*args)
    return by_collectives(*args)


def solution(mesh):
    mapped = jax.shard_map(
        on_device,
        mesh=mesh,
        in_specs=(
            P(("rep", "fs"), None, "tp"),
            P("fs", "tp"),
            P("fs", "tp"),
            P(None, "tp"),
            P("tp"),
            P("tp", "fs"),
            P(),
            P("fs", "tp"),
            P("fs", "tp"),
            P("tp", "fs"),
            P(),
        ),
        out_specs=P(("rep", "fs"), None, "tp"),
        check_vma=False,
    )
    return mapped
```

```python
import functools

import jax
import jax.numpy as jnp
from jax import lax
from jax.experimental import pallas as pl
from jax.experimental.pallas import tpu as pltpu
from jax.sharding import PartitionSpec as P

residual_scale = 2.0**0.25
epsilon = 1e-05


def normed(values):
    average = jnp.mean(values, axis=-1, keepdims=True)
    second = jnp.mean(values * values, axis=-1, keepdims=True)
    return (values - average) * lax.rsqrt(second - average * average + epsilon)


def interleave(left, right, parts):
    rows, width = left.shape
    pair = jnp.concatenate(
        (left.reshape(rows, parts, width // parts), right.reshape(rows, parts, width // parts)),
        axis=2,
    )
    return pair.reshape(rows, 2 * width)


def by_collectives(
    tokens,
    lin_weight,
    glu_weight,
    conv_taps,
    conv_gain,
    conv_out_weight,
    mix_gain,
    ff_gate,
    ff_up,
    ff_down,
    out_gain,
):
    n_fs, n_tp = lax.axis_size("fs"), lax.axis_size("tp")
    fs_index, tp_index = lax.axis_index("fs"), lax.axis_index("tp")
    seqs, length, feat = tokens.shape
    groups = n_fs * seqs
    rows = groups * length
    model = feat * n_tp
    conv_gain_all = lax.all_gather(conv_gain, "tp", axis=0, tiled=True)

    gathered = lax.all_gather(tokens, ("fs", "tp"), axis=0, tiled=False)
    all_tokens = (
        gathered.reshape(n_fs, n_tp, seqs, length, feat)
        .transpose(0, 2, 3, 1, 4)
        .reshape(rows, model)
    )
    glu_pair = lax.all_to_all(
        interleave(lin_weight, glu_weight, n_fs), "fs", split_axis=1, concat_axis=0, tiled=True
    )
    own_out = lax.all_to_all(conv_out_weight, "tp", split_axis=1, concat_axis=0, tiled=True)
    ff_pair = lax.all_to_all(
        interleave(ff_gate, ff_up, n_fs), "fs", split_axis=1, concat_axis=0, tiled=True
    )
    own_down = lax.all_to_all(ff_down, "fs", split_axis=0, concat_axis=1, tiled=True)

    chans = glu_pair.shape[1] // 2
    product = jnp.dot(all_tokens, glu_pair, preferred_element_type=jnp.float32)
    glu = (product[:, :chans] * jax.nn.sigmoid(product[:, chans:])).astype(jnp.bfloat16)
    n_taps = conv_taps.shape[0]
    margin = (n_taps - 1) // 2
    own_taps = lax.dynamic_slice_in_dim(conv_taps, fs_index * chans, chans, 1)
    padded = jnp.pad(
        glu.astype(jnp.float32).reshape(groups, length, chans),
        ((0, 0), (margin, margin), (0, 0)),
    )
    conv = sum(padded[:, k : k + length] * own_taps[k] for k in range(n_taps))
    conv = conv.reshape(rows, chans).astype(jnp.bfloat16)
    conv_all = lax.all_gather(conv, ("tp", "fs"), axis=1, tiled=True)
    activated = jax.nn.silu(normed(conv_all.astype(jnp.float32)) * conv_gain_all).astype(
        jnp.bfloat16
    )
    mixed_own = jnp.dot(activated, own_out, preferred_element_type=jnp.float32).astype(
        jnp.bfloat16
    )
    mixed = lax.all_gather(mixed_own, ("fs", "tp"), axis=1, tiled=True)
    before = residual_scale * all_tokens.astype(jnp.float32) + mixed.astype(jnp.float32)
    middle = (normed(before) * mix_gain).astype(jnp.bfloat16)

    units = ff_pair.shape[1] // 2
    both = jnp.dot(middle, ff_pair, preferred_element_type=jnp.float32)
    hidden = (jax.nn.silu(both[:, :units]) * both[:, units:]).astype(jnp.bfloat16)
    down = jnp.dot(hidden, own_down, preferred_element_type=jnp.float32).astype(jnp.bfloat16)
    sends = (
        down.reshape(n_fs, seqs * length, n_tp, feat)
        .transpose(0, 2, 1, 3)
        .reshape(n_fs * n_tp, seqs * length, feat)
    )
    arrived = lax.all_to_all(sends, ("fs", "tp"), split_axis=0, concat_axis=0, tiled=True)
    forward = jnp.sum(arrived.astype(jnp.float32), axis=0)
    forward = forward.astype(jnp.bfloat16).astype(jnp.float32)
    middle_own = lax.dynamic_slice(
        middle,
        (fs_index * seqs * length, tp_index * feat),
        (seqs * length, feat),
    )
    final = residual_scale * middle_own.astype(jnp.float32) + forward
    sums, squares = lax.psum(
        (jnp.sum(final, axis=1, keepdims=True), jnp.sum(final * final, axis=1, keepdims=True)),
        "tp",
    )
    average = sums / model
    out = (final - average) * lax.rsqrt(squares / model - average * average + epsilon)
    gain = lax.dynamic_slice_in_dim(out_gain, tp_index * feat, feat, 0)
    return (out * gain).astype(jnp.bfloat16).reshape(seqs, length, feat)


MESH = pl.DeviceIdType.MESH
LANES = 128
FIRST = ((2, 0), (3, 0))
CROSS = ((2, 1), (3, 1))
NEAR = ((1, 0), (1, 1), (0, 1))
OTHERS = FIRST + CROSS + NEAR
G, U, D = 0, 1, 2
INNER = {
    "t0": ((1, G, 2, 0), (1, G, 3, 0),),
    "t3": ((1, U, 2, 0),),
    "t5": ((1, U, 3, 0), (1, G, 1, 0),),
    "t6": ((1, G, 1, 1),),
    "t7": ((1, G, 0, 1), (1, G, 2, 1),),
    "c0": ((1, G, 3, 1),),
    "c2": ((0, G, 3, 0), (1, U, 1, 0),),
    "c3": ((1, U, 2, 1), (1, U, 3, 1),),
    "c4": ((0, G, 2, 0), (0, U, 3, 0), (1, U, 1, 1),),
    "c6": ((0, G, 1, 0), (0, U, 2, 0),),
    "c7": ((1, U, 0, 1), (1, D, 2, 0), (0, G, 0, 1),),
    "m0": ((1, D, 3, 0), (0, G, 3, 1), (0, G, 2, 1),),
    "m1": ((0, U, 3, 1), (0, U, 2, 1),),
    "m2": ((0, U, 1, 0), (0, U, 0, 1),),
    "m3": ((0, G, 1, 1),),
    "m4": ((1, D, 1, 0), (0, U, 1, 1),),
    "m5": ((1, D, 2, 1), (1, D, 3, 1), (1, D, 1, 1),),
    "m6": ((0, D, 2, 0),),
    "m7": ((0, D, 3, 0), (1, D, 0, 1),),
    "w2": ((0, D, 3, 1), (0, D, 2, 1),),
}
OUTER = {
    "t3": ((1, G, 2, 0), (1, G, 3, 0),),
    "t5": ((1, U, 2, 0), (1, G, 1, 0),),
    "t7": ((1, G, 0, 1),),
    "c0": ((1, U, 3, 0),),
    "c2": ((0, G, 2, 0),),
    "c3": ((1, G, 2, 1), (1, G, 3, 1),),
    "c4": ((0, U, 2, 0), (0, G, 3, 0), (0, G, 1, 0),),
    "c5": ((1, U, 2, 1), (1, U, 3, 1),),
    "c6": ((0, U, 3, 0), (0, G, 1, 1),),
    "c7": ((1, U, 0, 1), (1, U, 1, 0), (1, G, 1, 1), (0, G, 0, 1),),
    "m0": ((1, U, 1, 1), (0, G, 2, 1), (0, G, 3, 1),),
    "m1": ((0, U, 2, 1),),
    "m2": ((0, U, 3, 1),),
    "m3": ((1, D, 2, 0), (0, U, 1, 0), (0, U, 0, 1),),
    "m4": ((0, U, 1, 1),),
    "m5": ((1, D, 3, 0), (1, D, 2, 1), (1, D, 3, 1),),
    "m7": ((0, D, 2, 0), (1, D, 1, 0), (1, D, 1, 1), (1, D, 0, 1),),
    "m8": ((0, D, 3, 0),),
    "w2": ((0, D, 3, 1), (0, D, 2, 1),),
}

def fused(
    n_fs,
    n_tp,
    width,
    narrow,
    tok,
    lin_hbm,
    glu_hbm,
    taps_hbm,
    gain,
    out_weight,
    mix_gain,
    gate_hbm,
    up_hbm,
    down_hbm,
    out_gain,
    out,
    x_s,
    lin_s,
    gl_s,
    taps_s,
    mix_s,
    glu_s,
    gain_s,
    proj_s,
    pad_s,
    conv_s,
    norm_s,
    act_s,
    mixed_s,
    mid_s,
    gate_s,
    up_s,
    down_s,
    ff_s,
    hid_s,
    part_s,
    half_s,
    sum_s,
    z_s,
    y_s,
    stat_s,
    glu_sems,
    glu_cross_sems,
    small_sems,
    tok_sems,
    conv_sems,
    mixed_sems,
    ff_sems,
    cross_sems,
    local_sems,
    half_sems,
    z_sems,
    y_sems,
):
    rep, f, t = lax.axis_index("rep"), lax.axis_index("fs"), lax.axis_index("tp")
    other = 1 - t
    n_hi = n_fs // 2
    hi, lo = f // 2, f % 2
    rows, feat = x_s.shape[1:]
    length = rows // n_fs
    model = feat * n_tp
    depth = gate_hbm.shape[0]
    half_depth = depth // 2
    chans = LANES // 2
    pending = []

    def flip(z, step):
        return z + step - 2 * step * ((z // step) % 2)

    def along(k):
        z = hi
        for step in (1, 2):
            if k[0] & step:
                z = flip(z, step)
        return z * 2 + (1 - lo if k[1] else lo)

    def code(k):
        return k[0] * 2 + k[1]

    barrier = pltpu.get_barrier_semaphore()
    for k in OTHERS:
        pl.semaphore_signal(barrier, inc=1, device_id=(rep, along(k), t), device_id_type=MESH)
    pl.semaphore_signal(barrier, inc=1, device_id=(rep, f, other), device_id_type=MESH)
    pl.semaphore_signal(barrier, inc=1, device_id=(1 - rep, f, t), device_id_type=MESH)

    def rows_of(i):
        return pl.ds(pl.multiple_of(i * length, length), length)

    def depth_of(i, part, size):
        return pl.ds(pl.multiple_of(i * depth + part * half_depth, half_depth), size)

    def tok_slot(i, j):
        return x_s.at[j, rows_of(i)]

    per_half = n_fs // 2

    def start_of(i):
        return pl.multiple_of((i * (width // LANES) - i // per_half) * LANES, LANES)

    def is_short(i):
        return i % per_half == per_half - 1

    def sized(i, action):
        @pl.when(jnp.logical_not(is_short(i)))
        def _():
            action(width)

        @pl.when(is_short(i))
        def _():
            action(narrow)

    fetches = [
        pltpu.make_async_copy(src, dst, local_sems.at[n])
        for n, (src, dst) in enumerate(
            (
                (tok, tok_slot(f, t)),
                (lin_hbm, lin_s),
                (glu_hbm, gl_s),
                (taps_hbm, taps_s),
            )
        )
    ]
    for copy in fetches:
        copy.start()

    def own_copy(which, size):
        first = start_of(f)
        src, dst = (
            (gate_hbm.at[:, pl.ds(first, size)], gate_s.at[depth_of(f, 0, depth), pl.ds(0, size)]),
            (up_hbm.at[:, pl.ds(first, size)], up_s.at[depth_of(f, 0, depth), pl.ds(0, size)]),
            (down_hbm.at[pl.ds(first, size)], down_s.at[f, pl.ds(0, size)]),
        )[which]
        return pltpu.make_async_copy(src, dst, local_sems.at[4 + which])

    for which in range(3):
        sized(f, lambda size, which=which: own_copy(which, size).start())

    @pl.when(is_short(f))
    def _():
        gate_s[:, narrow:] = jnp.zeros((n_fs * depth, width - narrow), jnp.bfloat16)
        up_s[:, narrow:] = jnp.zeros((n_fs * depth, width - narrow), jnp.bfloat16)
        down_s[:, narrow:, :] = jnp.zeros((n_fs, width - narrow, down_s.shape[2]), jnp.bfloat16)

    def remote(src, dst, sems, index, device):
        return pltpu.make_async_remote_copy(
            src_ref=src,
            dst_ref=dst,
            send_sem=sems.at[0, index],
            recv_sem=sems.at[1, index],
            device_id=device,
            device_id_type=MESH,
        )

    def send(*parts):
        copy = remote(*parts)
        copy.start()
        pending.append(copy.wait_send)

    partner = (rep, f, other)
    mirror = (1 - rep, f, t)
    beside = (rep, along((0, 1)), t)
    close = (rep, along((1, 0)), t)
    far = (rep, along((2, 0)), t)

    def receive(dst, sems, index):
        remote(dst, dst, sems, index, partner).wait_recv()

    def gather_start(slot, sems):
        block = slot(f, t)
        send(block, block, sems, 0, far)
        send(block, block, sems, 1, close)
        send(block, block, sems, 3, beside)
        send(block, block, sems, 7, partner)

    inner = (hi % n_hi) // (n_hi // 2) != hi % 2

    def slot(name):
        for role, table in ((inner, INNER), (jnp.logical_not(inner), OUTER)):
            steps = table.get(name, ())

            @pl.when(role)
            def _(steps=steps):
                for send_it, which, *k in steps:
                    (weight_send if send_it else weight_forward)(which, tuple(k))

    def gather_finish(place, sems, name, between=None):
        between = between or {}

        def pause(step):
            slot(name + str(step))
            if step in between:
                between[step]()

        def got(index, k):
            block = place(along(k), t)
            receive(block, sems, index)
            return block

        block = got(3, (0, 1))
        send(block, block, sems, 7 + code((0, 1)), partner)
        pause(1)
        block = got(0, (2, 0))
        send(block, block, sems, 2, close)
        send(block, block, sems, 5, beside)
        send(block, block, sems, 7 + code((2, 0)), partner)
        pause(2)
        block = got(1, (1, 0))
        send(block, block, sems, 4, beside)
        send(block, block, sems, 7 + code((1, 0)), partner)
        pause(3)
        block = got(4, (1, 1))
        send(block, block, sems, 7 + code((1, 1)), partner)
        pause(4)
        block = got(2, (3, 0))
        send(block, block, sems, 6, beside)
        send(block, block, sems, 7 + code((3, 0)), partner)
        pause(5)
        block = got(5, (2, 1))
        send(block, block, sems, 7 + code((2, 1)), partner)
        pause(6)
        block = got(6, (3, 1))
        send(block, block, sems, 7 + code((3, 1)), partner)
        pause(7)
        for k in ((0, 0),) + OTHERS:
            receive(place(along(k), other), sems, 7 + code(k))

    half_width = width // 2

    def piece(which, to, source, part, size):
        first = start_of(to)
        ups = pl.ds(pl.multiple_of(part * half_depth, half_depth), half_depth)
        spot = depth_of(source, part, half_depth)
        deep = pl.ds(pl.multiple_of(part * (size // 2), size // 2), size // 2)
        from_down = pl.ds(pl.multiple_of(first + part * (size // 2), LANES // 2), size // 2)
        return (
            (gate_hbm.at[ups, pl.ds(first, size)], gate_s.at[spot, pl.ds(0, size)]),
            (up_hbm.at[ups, pl.ds(first, size)], up_s.at[spot, pl.ds(0, size)]),
            (down_hbm.at[from_down], down_s.at[source, deep]),
        )[which]

    def whole(which, k):
        return which == D and k in NEAR

    def weight_copy(which, k, size):
        to = along(k)
        if whole(which, k):
            src, dst = down_hbm.at[pl.ds(start_of(to), size)], down_s.at[f, pl.ds(0, size)]
        else:
            src, dst = piece(which, to, f, rep, size)
        return remote(src, dst, ff_sems, which * n_fs + code(k), (rep, to, t))

    def weight_send(which, k):
        sized(along(k), lambda size: weight_copy(which, k, size).start())

    def cross_copy(which, k, size):
        block = piece(which, f, along(k), rep, size)[1]
        return remote(block, block, cross_sems, which * n_fs + code(k), mirror)

    def weight_forward(which, k):
        def action(size):
            block = piece(which, f, along(k), rep, size)[1]
            receive(block, ff_sems, which * n_fs + code(k))
            cross_copy(which, k, size).start()

        sized(f, action)

    def weight_finish(which, ks):
        for k in ks:
            index = which * n_fs + code(k)

            def action(size):
                if whole(which, k):
                    receive(down_s.at[along(k), pl.ds(0, size)], ff_sems, index)
                else:
                    receive(piece(which, f, along(k), 1 - rep, size)[1], cross_sems, index)

            sized(f, action)

    pl.semaphore_wait(barrier, n_fs + 1)
    fetches[0].wait()
    gather_start(tok_slot, tok_sems)
    fetches[1].wait()
    fetches[2].wait()
    for d in range(n_fs):
        cols = slice(d * chans, (d + 1) * chans)
        mix_s[d] = jnp.concatenate((lin_s[:, cols], gl_s[:, cols]), axis=1)

    def glu_piece(source, part):
        return glu_s.at[depth_of(source, part, half_depth)]

    for k in OTHERS:
        to = along(k)
        own_rows = pl.ds(pl.multiple_of(rep * half_depth, half_depth), half_depth)
        send(mix_s.at[to, own_rows], glu_piece(f, rep), glu_sems, code(k), (rep, to, t))
    slot("t0")
    columns = pl.ds(pl.multiple_of(other * LANES, LANES), LANES)
    own_columns = pl.ds(pl.multiple_of(t * LANES, LANES), LANES)
    send(gain, gain_s.at[t], small_sems, 0, partner)
    send(out_weight.at[:, columns], proj_s.at[t], small_sems, 1, partner)

    glu_s[pl.ds(pl.multiple_of(f * depth, depth), depth), :] = mix_s[f]
    gain_s[t] = gain[...]
    proj_s[t] = out_weight[:, own_columns]
    pad_s[...] = jnp.zeros_like(pad_s)

    def glu_forward(ks):
        for k in ks:
            block = glu_piece(along(k), rep)
            receive(block, glu_sems, code(k))
            send(block, block, glu_cross_sems, code(k), mirror)

    gather_finish(
        tok_slot,
        tok_sems,
        "t",
        {
            4: lambda: glu_forward(NEAR),
            5: lambda: glu_forward(FIRST),
            6: lambda: glu_forward(CROSS),
        },
    )
    for k in OTHERS:
        receive(glu_piece(along(k), 1 - rep), glu_cross_sems, code(k))

    product = sum(
        jnp.dot(
            x_s[j], glu_s[j * feat : (j + 1) * feat], preferred_element_type=jnp.float32
        )
        for j in range(n_tp)
    )
    glu = product[:, :chans] / (1.0 + jnp.exp(-product[:, chans:]))
    top = rows // 2
    packed = jnp.concatenate((glu[:top], glu[top:]), axis=1)
    packed = packed.astype(jnp.bfloat16).astype(jnp.float32)
    fetches[3].wait()
    lanes = lax.broadcasted_iota(jnp.int32, (1, LANES), 1)
    tap_pair = taps_s[:, pl.ds(pl.multiple_of(f // 2 * LANES, LANES), LANES)]
    turned = pltpu.roll(tap_pair, chans, 1)
    taps = jnp.where((lanes < chans) == (f % 2 == 0), tap_pair, turned)
    n_taps = taps.shape[0]
    margin = (n_taps - 1) // 2
    slot("d0")
    conv_slot = lambda i, j: conv_s.at[j * n_fs + i]
    groups = n_fs // 2
    for g in range(groups):
        pad_s[g, 16 : 16 + length, :] = packed[g * length : (g + 1) * length]
    for g in range(groups):
        acc = jnp.zeros((length, LANES), jnp.float32)
        for k in range(n_taps):
            first = 16 - margin + k
            acc = acc + pad_s[g, first : first + length, :] * taps[k : k + 1, :]
        conv_s[t * n_fs + f, g * length : (g + 1) * length, :] = acc.astype(jnp.bfloat16)
    gather_start(conv_slot, conv_sems)
    slot("c0")
    gather_finish(conv_slot, conv_sems, "c")
    receive(gain_s.at[other], small_sems, 0)
    receive(proj_s.at[other], small_sems, 1)

    for j in range(n_fs * n_tp // 2):
        left = conv_s[2 * j].astype(jnp.float32)
        right = conv_s[2 * j + 1].astype(jnp.float32)
        cols = slice(j * LANES, (j + 1) * LANES)
        norm_s[:top, cols] = jnp.concatenate((left[:, :chans], right[:, :chans]), axis=1)
        norm_s[top:, cols] = jnp.concatenate((left[:, chans:], right[:, chans:]), axis=1)
    gains = jnp.concatenate([gain_s[j] for j in range(n_tp)], axis=1)

    @pl.loop(0, n_fs)
    def _(i):
        here = rows_of(i)
        v = normed(norm_s[here, :]) * gains
        act_s[here, :] = (v / (1.0 + jnp.exp(-v))).astype(jnp.bfloat16)

    slot("n0")
    share = proj_s.shape[1]
    mixed_slot = lambda i, j: mixed_s.at[i * n_tp + j]
    mixed_s[f * n_tp + t] = sum(
        jnp.dot(
            act_s[:, j * share : (j + 1) * share],
            proj_s[j],
            preferred_element_type=jnp.float32,
        )
        for j in range(n_tp)
    ).astype(jnp.bfloat16)
    gather_start(mixed_slot, mixed_sems)
    slot("m0")
    gather_finish(mixed_slot, mixed_sems, "m")
    slot("m8")

    @pl.loop(0, n_fs)
    def _(i):
        here = rows_of(i)
        skip = jnp.concatenate([x_s[j, here, :] for j in range(n_tp)], axis=1)
        added = jnp.concatenate([mixed_s[j, here, :] for j in range(n_fs * n_tp)], axis=1)
        before = residual_scale * skip.astype(jnp.float32) + added.astype(jnp.float32)
        mid_s[here, :] = (normed(before) * mix_gain[...]).astype(jnp.bfloat16)

    slot("e0")
    near_side = hi // (n_hi // 2)
    deep = n_fs // n_tp * depth

    def partial_ff(side):
        inner_rows = pl.ds(pl.multiple_of(side * deep, deep), deep)
        left = mid_s[:, inner_rows]
        return tuple(
            jnp.dot(left, right[inner_rows, :], preferred_element_type=jnp.float32)
            for right in (gate_s, up_s)
        )

    for which in (0, 1):
        sized(f, lambda size: own_copy(which, size).wait())
        weight_finish(which, NEAR)
        slot("w" + str(which))
    ff_s[0], ff_s[1] = partial_ff(near_side)
    slot("w2")
    for i, (which, ks) in enumerate(((0, FIRST), (1, FIRST), (0, CROSS), (1, CROSS))):
        weight_finish(which, ks)
        slot("w" + str(3 + i))

    gate, upward = partial_ff(1 - near_side)
    gate, upward = gate + ff_s[0], upward + ff_s[1]
    hid_s[...] = (gate / (1.0 + jnp.exp(-gate)) * upward).astype(jnp.bfloat16)
    slot("g0")

    sized(f, lambda size: own_copy(2, size).wait())
    weight_finish(2, NEAR)
    slot("g2")
    span = down_s.shape[2]
    per_core = n_fs // n_tp
    steps = (3, 2, 1, 0)

    def project(side):
        @pl.loop(0, per_core)
        def _(j):
            part_s[side, :, pl.ds(pl.multiple_of(j * span, span), span)] = jnp.dot(
                hid_s[...], down_s[side * per_core + j], preferred_element_type=jnp.float32
            ).astype(jnp.bfloat16)

    def half_copy(k):
        here = rows_of(along(k))
        return remote(part_s.at[other, here], half_s.at[here], half_sems, code(k), partner)

    def hand_over():
        for low in (1, 0):
            for d in steps:
                half_copy((d, low)).start()

    def joined(k):
        here = rows_of(along(k))
        receive(half_s.at[here], half_sems, code(k))
        return part_s[t, here, :].astype(jnp.float32) + half_s[here, :].astype(jnp.float32)

    def aside_copy(d):
        return remote(sum_s.at[rows_of(along((d, 1)))], y_s.at[d], y_sems, d, beside)

    def aside():
        for d in steps:
            sum_s[rows_of(along((d, 1))), :] = joined((d, 1)).astype(jnp.bfloat16)
            aside_copy(d).start()

    project(near_side)
    pl.when(t == near_side)(aside)
    pl.when(t != near_side)(hand_over)
    slot("g3")
    weight_finish(2, FIRST + CROSS)
    project(1 - near_side)
    pl.when(t == near_side)(hand_over)
    pl.when(t != near_side)(aside)
    for d in steps:
        pending.append(aside_copy(d).wait_send)
        for low in (0, 1):
            pending.append(half_copy((d, low)).wait_send)

    for d in steps:
        here = rows_of(along((d, 0)))
        forward = joined((d, 0))
        receive(y_s.at[d], y_sems, d)
        forward = forward + y_s[d].astype(jnp.float32)
        if d % 2:
            sum_s[here, :] = forward.astype(jnp.bfloat16)
            send(sum_s.at[here], z_s.at[d // 2], z_sems, d // 2, close)
        elif d:
            receive(z_s.at[1], z_sems, 1)
            sum_s[here, :] = (forward + z_s[1].astype(jnp.float32)).astype(jnp.bfloat16)
            send(sum_s.at[here], z_s.at[2], z_sems, 2, far)
    for i in (0, 2):
        receive(z_s.at[i], z_sems, i)
        forward = forward + z_s[i].astype(jnp.float32)
    forward = forward.astype(jnp.bfloat16).astype(jnp.float32)
    own_half = pl.ds(pl.multiple_of(t * feat, feat), feat)
    final = residual_scale * mid_s[rows_of(f), own_half].astype(jnp.float32) + forward
    lane = lax.broadcasted_iota(jnp.int32, (length, LANES), 1)
    stat_s[t] = jnp.where(
        lane == 0,
        jnp.sum(final, axis=1, keepdims=True),
        jnp.sum(final * final, axis=1, keepdims=True),
    )
    send(stat_s.at[t], stat_s.at[t], small_sems, 2, partner)
    receive(stat_s.at[other], small_sems, 2)
    stats = (stat_s[0] + stat_s[1]) / model
    average, second = stats[:, 0:1], stats[:, 1:2]
    scaled = (final - average) * lax.rsqrt(second - average * average + epsilon)
    out[...] = (scaled * out_gain[t]).astype(jnp.bfloat16)
    for wait in pending:
        wait()
    for which in range(3):
        for k in OTHERS:
            sized(along(k), lambda size: weight_copy(which, k, size).wait_send())
            if not whole(which, k):
                sized(f, lambda size: cross_copy(which, k, size).wait_send())


def by_kernel(
    tokens,
    lin_weight,
    glu_weight,
    conv_taps,
    conv_gain,
    conv_out_weight,
    mix_gain,
    ff_gate,
    ff_up,
    ff_down,
    out_gain,
):
    n_fs, n_tp = lax.axis_size("fs"), lax.axis_size("tp")
    _, length, feat = tokens.shape
    rows, model = n_fs * length, feat * n_tp
    depth, own_chans = lin_weight.shape
    chans = own_chans // n_fs
    width, narrow = widths(ff_gate.shape[1], n_fs)
    vmem, far = pl.BlockSpec(memory_space=pltpu.VMEM), pl.BlockSpec(memory_space=pl.ANY)
    bf, fl = jnp.bfloat16, jnp.float32
    span = ff_down.shape[1]
    pair = lambda n: pltpu.SemaphoreType.DMA((2, n))
    result = pl.pallas_call(
        functools.partial(fused, n_fs, n_tp, width, narrow),
        out_shape=jax.ShapeDtypeStruct((length, feat), bf),
        in_specs=[far] * 4 + [vmem] * 3 + [far] * 3 + [vmem],
        out_specs=vmem,
        scratch_shapes=[
            pltpu.VMEM((n_tp, rows, feat), bf),
            pltpu.VMEM((depth, own_chans), bf),
            pltpu.VMEM((depth, own_chans), bf),
            pltpu.VMEM(conv_taps.shape, fl),
            pltpu.VMEM((n_fs, depth, 2 * chans), bf),
            pltpu.VMEM((n_fs * depth, 2 * chans), bf),
            pltpu.VMEM((n_tp, 1, own_chans), fl),
            pltpu.VMEM((n_tp, own_chans, span // n_tp), bf),
            pltpu.VMEM((n_fs // 2, length + 32, LANES), fl),
            pltpu.VMEM((n_fs * n_tp, rows // 2, LANES), bf),
            pltpu.VMEM((rows, own_chans * n_tp), fl),
            pltpu.VMEM((rows, own_chans * n_tp), bf),
            pltpu.VMEM((n_fs * n_tp, rows, LANES), bf),
            pltpu.VMEM((rows, model), bf),
            pltpu.VMEM((n_fs * depth, width), bf),
            pltpu.VMEM((n_fs * depth, width), bf),
            pltpu.VMEM((n_fs, width, span), bf),
            pltpu.VMEM((2, rows, width), fl),
            pltpu.VMEM((rows, width), bf),
            pltpu.VMEM((n_tp, rows, feat), bf),
            pltpu.VMEM((rows, feat), bf),
            pltpu.VMEM((rows, feat), bf),
            pltpu.VMEM((3, length, feat), bf),
            pltpu.VMEM((n_fs // 2, length, feat), bf),
            pltpu.VMEM((n_tp, length, LANES), fl),
            pair(n_fs),
            pair(n_fs),
            pair(3),
            pair(2 * n_fs),
            pair(2 * n_fs),
            pair(2 * n_fs),
            pair(3 * n_fs),
            pair(3 * n_fs),
            pltpu.SemaphoreType.DMA((7,)),
            pair(n_fs),
            pair(3),
            pair(n_fs // 2),
        ],
        compiler_params=pltpu.CompilerParams(
            collective_id=0, has_side_effects=True, vmem_limit_bytes=60 * 2**20
        ),
    )(
        tokens[0],
        lin_weight,
        glu_weight,
        conv_taps,
        conv_gain[None],
        conv_out_weight,
        mix_gain[None],
        ff_gate,
        ff_up,
        ff_down,
        out_gain.reshape(n_tp, 1, feat),
    )
    return result[None]


def widths(units, n_fs):
    half = n_fs // 2
    blocks = units // LANES // 2
    most = -(-blocks // half)
    return most * LANES, (blocks - most * (half - 1)) * LANES


def on_device(*args):
    tokens, lin_weight, conv_out_weight, ff_gate = args[0], args[1], args[5], args[7]
    n_fs, n_tp, n_rep = (lax.axis_size(a) for a in ("fs", "tp", "rep"))
    seqs, length, feat = tokens.shape
    units = ff_gate.shape[1]
    width, narrow = widths(units, n_fs)
    fits = (
        n_rep == 2
        and n_tp == 2
        and n_fs == 8
        and seqs == 1
        and length % 16 == 0
        and args[3].shape[0] <= 33
        and lin_weight.shape[1] * 2 == n_fs * LANES
        and conv_out_weight.shape[1] == n_tp * LANES
        and feat % LANES == 0
        and units % (2 * LANES) == 0
        and narrow == width - LANES > 0
        and lin_weight.shape[0] % 32 == 0
    )
    if fits:
        return by_kernel(*args)
    return by_collectives(*args)


def solution(mesh):
    mapped = jax.shard_map(
        on_device,
        mesh=mesh,
        in_specs=(
            P(("rep", "fs"), None, "tp"),
            P("fs", "tp"),
            P("fs", "tp"),
            P(None, "tp"),
            P("tp"),
            P("tp", "fs"),
            P(),
            P("fs", "tp"),
            P("fs", "tp"),
            P("tp", "fs"),
            P(),
        ),
        out_specs=P(("rep", "fs"), None, "tp"),
        check_vma=False,
    )
    return mapped
```

```python
import functools

import jax
import jax.numpy as jnp
from jax import lax
from jax.experimental import pallas as pl
from jax.experimental.pallas import tpu as pltpu
from jax.sharding import PartitionSpec as P

residual_scale = 2.0**0.25
epsilon = 1e-05


def normed(values):
    average = jnp.mean(values, axis=-1, keepdims=True)
    second = jnp.mean(values * values, axis=-1, keepdims=True)
    return (values - average) * lax.rsqrt(second - average * average + epsilon)


def interleave(left, right, parts):
    rows, width = left.shape
    pair = jnp.concatenate(
        (left.reshape(rows, parts, width // parts), right.reshape(rows, parts, width // parts)),
        axis=2,
    )
    return pair.reshape(rows, 2 * width)


def by_collectives(
    tokens,
    lin_weight,
    glu_weight,
    conv_taps,
    conv_gain,
    conv_out_weight,
    mix_gain,
    ff_gate,
    ff_up,
    ff_down,
    out_gain,
):
    n_fs, n_tp = lax.axis_size("fs"), lax.axis_size("tp")
    fs_index, tp_index = lax.axis_index("fs"), lax.axis_index("tp")
    seqs, length, feat = tokens.shape
    groups = n_fs * seqs
    rows = groups * length
    model = feat * n_tp
    conv_gain_all = lax.all_gather(conv_gain, "tp", axis=0, tiled=True)

    gathered = lax.all_gather(tokens, ("fs", "tp"), axis=0, tiled=False)
    all_tokens = (
        gathered.reshape(n_fs, n_tp, seqs, length, feat)
        .transpose(0, 2, 3, 1, 4)
        .reshape(rows, model)
    )
    glu_pair = lax.all_to_all(
        interleave(lin_weight, glu_weight, n_fs), "fs", split_axis=1, concat_axis=0, tiled=True
    )
    own_out = lax.all_to_all(conv_out_weight, "tp", split_axis=1, concat_axis=0, tiled=True)
    ff_pair = lax.all_to_all(
        interleave(ff_gate, ff_up, n_fs), "fs", split_axis=1, concat_axis=0, tiled=True
    )
    own_down = lax.all_to_all(ff_down, "fs", split_axis=0, concat_axis=1, tiled=True)

    chans = glu_pair.shape[1] // 2
    product = jnp.dot(all_tokens, glu_pair, preferred_element_type=jnp.float32)
    glu = (product[:, :chans] * jax.nn.sigmoid(product[:, chans:])).astype(jnp.bfloat16)
    n_taps = conv_taps.shape[0]
    margin = (n_taps - 1) // 2
    own_taps = lax.dynamic_slice_in_dim(conv_taps, fs_index * chans, chans, 1)
    padded = jnp.pad(
        glu.astype(jnp.float32).reshape(groups, length, chans),
        ((0, 0), (margin, margin), (0, 0)),
    )
    conv = sum(padded[:, k : k + length] * own_taps[k] for k in range(n_taps))
    conv = conv.reshape(rows, chans).astype(jnp.bfloat16)
    conv_all = lax.all_gather(conv, ("tp", "fs"), axis=1, tiled=True)
    activated = jax.nn.silu(normed(conv_all.astype(jnp.float32)) * conv_gain_all).astype(
        jnp.bfloat16
    )
    mixed_own = jnp.dot(activated, own_out, preferred_element_type=jnp.float32).astype(
        jnp.bfloat16
    )
    mixed = lax.all_gather(mixed_own, ("fs", "tp"), axis=1, tiled=True)
    before = residual_scale * all_tokens.astype(jnp.float32) + mixed.astype(jnp.float32)
    middle = (normed(before) * mix_gain).astype(jnp.bfloat16)

    units = ff_pair.shape[1] // 2
    both = jnp.dot(middle, ff_pair, preferred_element_type=jnp.float32)
    hidden = (jax.nn.silu(both[:, :units]) * both[:, units:]).astype(jnp.bfloat16)
    down = jnp.dot(hidden, own_down, preferred_element_type=jnp.float32).astype(jnp.bfloat16)
    sends = (
        down.reshape(n_fs, seqs * length, n_tp, feat)
        .transpose(0, 2, 1, 3)
        .reshape(n_fs * n_tp, seqs * length, feat)
    )
    arrived = lax.all_to_all(sends, ("fs", "tp"), split_axis=0, concat_axis=0, tiled=True)
    forward = jnp.sum(arrived.astype(jnp.float32), axis=0)
    forward = forward.astype(jnp.bfloat16).astype(jnp.float32)
    middle_own = lax.dynamic_slice(
        middle,
        (fs_index * seqs * length, tp_index * feat),
        (seqs * length, feat),
    )
    final = residual_scale * middle_own.astype(jnp.float32) + forward
    sums, squares = lax.psum(
        (jnp.sum(final, axis=1, keepdims=True), jnp.sum(final * final, axis=1, keepdims=True)),
        "tp",
    )
    average = sums / model
    out = (final - average) * lax.rsqrt(squares / model - average * average + epsilon)
    gain = lax.dynamic_slice_in_dim(out_gain, tp_index * feat, feat, 0)
    return (out * gain).astype(jnp.bfloat16).reshape(seqs, length, feat)


MESH = pl.DeviceIdType.MESH
LANES = 128
FIRST = ((2, 0), (3, 0))
CROSS = ((2, 1), (3, 1))
NEAR = ((1, 0), (1, 1), (0, 1))
OTHERS = FIRST + CROSS + NEAR
G, U, D = 0, 1, 2
INNER = {
    "t0": ((1, G, 2, 0), (1, G, 3, 0), (1, G, 0, 1),),
    "t3": ((1, U, 2, 0),),
    "t5": ((1, U, 3, 0), (1, G, 1, 0),),
    "t6": ((1, G, 1, 1),),
    "t7": ((1, G, 2, 1), (1, D, 0, 1),),
    "c0": ((1, G, 3, 1),),
    "c2": ((0, G, 3, 0), (1, U, 1, 0),),
    "c3": ((1, U, 2, 1), (1, U, 3, 1),),
    "c4": ((0, G, 2, 0), (0, U, 3, 0), (1, U, 1, 1),),
    "c6": ((0, G, 1, 0), (0, U, 2, 0),),
    "c7": ((1, U, 0, 1), (1, D, 2, 0), (0, G, 0, 1),),
    "m0": ((1, D, 3, 0), (0, G, 3, 1), (0, G, 2, 1),),
    "m1": ((0, U, 3, 1), (0, U, 2, 1),),
    "m2": ((0, U, 1, 0), (0, U, 0, 1),),
    "m3": ((0, G, 1, 1),),
    "m4": ((1, D, 1, 0), (0, U, 1, 1),),
    "m5": ((1, D, 2, 1), (1, D, 3, 1), (1, D, 1, 1),),
    "m6": ((0, D, 2, 0),),
    "m7": ((0, D, 3, 0),),
    "w2": ((0, D, 3, 1), (0, D, 2, 1),),
}
OUTER = {
    "t3": ((1, G, 2, 0), (1, G, 3, 0),),
    "t5": ((1, U, 2, 0), (1, G, 1, 0),),
    "t7": ((1, D, 0, 1),),
    "c0": ((1, U, 3, 0),),
    "c2": ((0, G, 2, 0),),
    "c3": ((1, G, 2, 1), (1, G, 3, 1),),
    "c4": ((0, U, 2, 0), (0, G, 3, 0), (0, G, 1, 0),),
    "c5": ((1, U, 2, 1), (1, U, 3, 1),),
    "c6": ((0, U, 3, 0), (0, G, 1, 1),),
    "c7": ((1, U, 0, 1), (1, U, 1, 0), (1, G, 1, 1), (0, G, 0, 1),),
    "m0": ((1, U, 1, 1), (0, G, 2, 1), (0, G, 3, 1),),
    "m1": ((0, U, 2, 1),),
    "m2": ((0, U, 3, 1),),
    "m3": ((1, D, 2, 0), (0, U, 1, 0), (0, U, 0, 1),),
    "m4": ((0, U, 1, 1),),
    "m5": ((1, D, 3, 0), (1, D, 2, 1), (1, D, 3, 1),),
    "m7": ((0, D, 2, 0), (1, D, 1, 0), (1, D, 1, 1),),
    "m8": ((0, D, 3, 0),),
    "w2": ((0, D, 3, 1), (0, D, 2, 1),),
    "t0": ((1, G, 0, 1),),
}

def fused(
    n_fs,
    n_tp,
    width,
    narrow,
    tok,
    lin_hbm,
    glu_hbm,
    taps_hbm,
    gain,
    out_weight,
    mix_gain,
    gate_hbm,
    up_hbm,
    down_hbm,
    out_gain,
    out,
    x_s,
    lin_s,
    gl_s,
    taps_s,
    mix_s,
    glu_s,
    gain_s,
    proj_s,
    pad_s,
    conv_s,
    norm_s,
    act_s,
    mixed_s,
    mid_s,
    gate_s,
    up_s,
    down_s,
    ff_s,
    hid_s,
    part_s,
    half_s,
    sum_s,
    z_s,
    y_s,
    stat_s,
    out_s,
    glu_sems,
    glu_cross_sems,
    small_sems,
    tok_sems,
    conv_sems,
    mixed_sems,
    ff_sems,
    cross_sems,
    local_sems,
    half_sems,
    z_sems,
    y_sems,
):
    rep, f, t = lax.axis_index("rep"), lax.axis_index("fs"), lax.axis_index("tp")
    other = 1 - t
    n_hi = n_fs // 2
    hi, lo = f // 2, f % 2
    rows, feat = x_s.shape[1:]
    length = rows // n_fs
    model = feat * n_tp
    depth = gate_hbm.shape[0]
    half_depth = depth // 2
    chans = LANES // 2

    def flip(z, step):
        return z + step - 2 * step * ((z // step) % 2)

    def along(k):
        z = hi
        for step in (1, 2):
            if k[0] & step:
                z = flip(z, step)
        return z * 2 + (1 - lo if k[1] else lo)

    def code(k):
        return k[0] * 2 + k[1]

    barrier = pltpu.get_barrier_semaphore()
    for k in OTHERS:
        pl.semaphore_signal(barrier, inc=1, device_id=(rep, along(k), t), device_id_type=MESH)
    pl.semaphore_signal(barrier, inc=1, device_id=(rep, f, other), device_id_type=MESH)
    pl.semaphore_signal(barrier, inc=1, device_id=(1 - rep, f, t), device_id_type=MESH)

    def rows_of(i):
        return pl.ds(pl.multiple_of(i * length, length), length)

    def depth_of(i, part, size):
        return pl.ds(pl.multiple_of(i * depth + part * half_depth, half_depth), size)

    def tok_slot(i, j):
        return x_s.at[j, rows_of(i)]

    per_half = n_fs // 2

    def start_of(i):
        return pl.multiple_of((i * (width // LANES) - i // per_half) * LANES, LANES)

    def is_short(i):
        return i % per_half == per_half - 1

    def sized(i, action):
        @pl.when(jnp.logical_not(is_short(i)))
        def _():
            action(width)

        @pl.when(is_short(i))
        def _():
            action(narrow)

    fetches = [
        pltpu.make_async_copy(src, dst, local_sems.at[n])
        for n, (src, dst) in enumerate(
            (
                (tok, tok_slot(f, t)),
                (lin_hbm, lin_s),
                (glu_hbm, gl_s),
                (taps_hbm, taps_s),
            )
        )
    ]
    for copy in fetches:
        copy.start()

    def own_copy(which, size):
        first = start_of(f)
        src, dst = (
            (gate_hbm.at[:, pl.ds(first, size)], gate_s.at[depth_of(f, 0, depth), pl.ds(0, size)]),
            (up_hbm.at[:, pl.ds(first, size)], up_s.at[depth_of(f, 0, depth), pl.ds(0, size)]),
            (down_hbm.at[pl.ds(first, size)], down_s.at[f, pl.ds(0, size)]),
        )[which]
        return pltpu.make_async_copy(src, dst, local_sems.at[4 + which])

    for which in range(3):
        sized(f, lambda size, which=which: own_copy(which, size).start())

    @pl.when(is_short(f))
    def _():
        gate_s[:, narrow:] = jnp.zeros((n_fs * depth, width - narrow), jnp.bfloat16)
        up_s[:, narrow:] = jnp.zeros((n_fs * depth, width - narrow), jnp.bfloat16)
        down_s[:, narrow:, :] = jnp.zeros((n_fs, width - narrow, down_s.shape[2]), jnp.bfloat16)

    def remote(src, dst, send_sem, recv_sem, device):
        return pltpu.make_async_remote_copy(
            src_ref=src,
            dst_ref=dst,
            send_sem=send_sem,
            recv_sem=recv_sem,
            device_id=device,
            device_id_type=MESH,
        )

    def send(src, dst, sems, index, device):
        remote(src, dst, sems.at[0], sems.at[1 + index], device).start()

    partner = (rep, f, other)
    mirror = (1 - rep, f, t)
    beside = (rep, along((0, 1)), t)
    close = (rep, along((1, 0)), t)
    far = (rep, along((2, 0)), t)

    def arrive(dst, sem):
        remote(dst, dst, sem, sem, partner).wait_recv()

    def receive(dst, sems, index):
        arrive(dst, sems.at[1 + index])

    def sent(src, sem):
        remote(src, src, sem, sem, partner).wait_send()

    def small_copy(src, dst, index):
        return remote(src, dst, small_sems.at[index], small_sems.at[3 + index], partner)

    def gather_start(slot, sems):
        block = slot(f, t)
        send(block, block, sems, 0, far)
        send(block, block, sems, 1, close)
        send(block, block, sems, 3, beside)
        send(block, block, sems, 7, partner)

    inner = (hi % n_hi) // (n_hi // 2) != hi % 2

    def slot(name):
        for role, table in ((inner, INNER), (jnp.logical_not(inner), OUTER)):
            steps = table.get(name, ())

            @pl.when(role)
            def _(steps=steps):
                for send_it, which, *k in steps:
                    (weight_send if send_it else weight_forward)(which, tuple(k))

    def gather_finish(place, all_of, sems, name, between=None):
        between = between or {}

        def pause(step):
            slot(name + str(step))
            if step in between:
                between[step]()

        def got(index, k):
            block = place(along(k), t)
            receive(block, sems, index)
            return block

        block = got(3, (0, 1))
        send(block, block, sems, 7, partner)
        pause(1)
        block = got(0, (2, 0))
        send(block, block, sems, 2, close)
        send(block, block, sems, 5, beside)
        send(block, block, sems, 7, partner)
        pause(2)
        block = got(1, (1, 0))
        send(block, block, sems, 4, beside)
        send(block, block, sems, 7, partner)
        pause(3)
        block = got(4, (1, 1))
        send(block, block, sems, 7, partner)
        pause(4)
        block = got(2, (3, 0))
        send(block, block, sems, 6, beside)
        send(block, block, sems, 7, partner)
        pause(5)
        block = got(5, (2, 1))
        send(block, block, sems, 7, partner)
        pause(6)
        block = got(6, (3, 1))
        send(block, block, sems, 7, partner)
        pause(7)
        receive(all_of(other), sems, 7)

    half_width = width // 2

    def piece(which, to, source, part, size):
        first = start_of(to)
        ups = pl.ds(pl.multiple_of(part * half_depth, half_depth), half_depth)
        spot = depth_of(source, part, half_depth)
        deep = pl.ds(pl.multiple_of(part * (size // 2), size // 2), size // 2)
        from_down = pl.ds(pl.multiple_of(first + part * (size // 2), LANES // 2), size // 2)
        return (
            (gate_hbm.at[ups, pl.ds(first, size)], gate_s.at[spot, pl.ds(0, size)]),
            (up_hbm.at[ups, pl.ds(first, size)], up_s.at[spot, pl.ds(0, size)]),
            (down_hbm.at[from_down], down_s.at[source, deep]),
        )[which]

    def whole(which, k):
        return which == D and k in NEAR

    def weight_copy(which, k, size):
        to = along(k)
        if whole(which, k):
            src, dst = down_hbm.at[pl.ds(start_of(to), size)], down_s.at[f, pl.ds(0, size)]
        else:
            src, dst = piece(which, to, f, rep, size)
        return remote(
            src, dst, ff_sems.at[3 * n_fs + code(k)], ff_sems.at[which * n_fs + code(k)], (rep, to, t)
        )

    def weight_send(which, k):
        sized(along(k), lambda size: weight_copy(which, k, size).start())

    def group_sem(which, k):
        group = 0 if k in NEAR else 1 if k in FIRST else 2
        return cross_sems.at[2 + (6 if which == D else 3 * which + group)]

    def cross_copy(which, k, size):
        block = piece(which, f, along(k), rep, size)[1]
        return remote(block, block, cross_sems.at[which // 2], group_sem(which, k), mirror)

    def weight_forward(which, k):
        def action(size):
            block = piece(which, f, along(k), rep, size)[1]
            arrive(block, ff_sems.at[which * n_fs + code(k)])
            cross_copy(which, k, size).start()

        sized(f, action)

    def weight_finish(which, ks):
        def action(size):
            if whole(which, ks[0]):
                for k in ks:
                    arrive(down_s.at[along(k), pl.ds(0, size)], ff_sems.at[which * n_fs + code(k)])
            else:
                arrive(
                    gate_s.at[pl.ds(0, len(ks) * half_depth), pl.ds(0, size)],
                    group_sem(which, ks[0]),
                )

        sized(f, action)

    pl.semaphore_wait(barrier, n_fs + 1)
    fetches[0].wait()
    gather_start(tok_slot, tok_sems)
    fetches[1].wait()
    fetches[2].wait()
    for d in range(n_fs):
        cols = slice(d * chans, (d + 1) * chans)
        mix_s[d] = jnp.concatenate((lin_s[:, cols], gl_s[:, cols]), axis=1)

    def glu_piece(source, part):
        return glu_s.at[depth_of(source, part, half_depth)]

    for k in OTHERS:
        to = along(k)
        own_rows = pl.ds(pl.multiple_of(rep * half_depth, half_depth), half_depth)
        send(mix_s.at[to, own_rows], glu_piece(f, rep), glu_sems, code(k), (rep, to, t))
    slot("t0")
    columns = pl.ds(pl.multiple_of(other * LANES, LANES), LANES)
    own_columns = pl.ds(pl.multiple_of(t * LANES, LANES), LANES)
    small_copy(gain, gain_s.at[t], 0).start()
    small_copy(out_weight.at[:, columns], proj_s.at[t], 1).start()

    glu_s[pl.ds(pl.multiple_of(f * depth, depth), depth), :] = mix_s[f]
    gain_s[t] = gain[...]
    proj_s[t] = out_weight[:, own_columns]
    pad_s[...] = jnp.zeros_like(pad_s)

    def glu_forward(ks):
        for k in ks:
            block = glu_piece(along(k), rep)
            receive(block, glu_sems, code(k))
            send(block, block, glu_cross_sems, 0, mirror)

    gather_finish(
        tok_slot,
        lambda j: x_s.at[j],
        tok_sems,
        "t",
        {
            4: lambda: glu_forward(NEAR),
            5: lambda: glu_forward(FIRST),
            6: lambda: glu_forward(CROSS),
        },
    )
    seven = glu_s.at[pl.ds(0, len(OTHERS) * half_depth)]
    receive(seven, glu_cross_sems, 0)

    product = sum(
        jnp.dot(
            x_s[j], glu_s[j * feat : (j + 1) * feat], preferred_element_type=jnp.float32
        )
        for j in range(n_tp)
    )
    glu = product[:, :chans] / (1.0 + jnp.exp(-product[:, chans:]))
    top = rows // 2
    packed = jnp.concatenate((glu[:top], glu[top:]), axis=1)
    packed = packed.astype(jnp.bfloat16).astype(jnp.float32)
    fetches[3].wait()
    lanes = lax.broadcasted_iota(jnp.int32, (1, LANES), 1)
    tap_pair = taps_s[:, pl.ds(pl.multiple_of(f // 2 * LANES, LANES), LANES)]
    turned = pltpu.roll(tap_pair, chans, 1)
    taps = jnp.where((lanes < chans) == (f % 2 == 0), tap_pair, turned)
    n_taps = taps.shape[0]
    margin = (n_taps - 1) // 2
    slot("d0")
    conv_slot = lambda i, j: conv_s.at[j * n_fs + i]
    groups = n_fs // 2
    for g in range(groups):
        pad_s[g, 16 : 16 + length, :] = packed[g * length : (g + 1) * length]
    for g in range(groups):
        acc = jnp.zeros((length, LANES), jnp.float32)
        for k in range(n_taps):
            first = 16 - margin + k
            acc = acc + pad_s[g, first : first + length, :] * taps[k : k + 1, :]
        conv_s[t * n_fs + f, g * length : (g + 1) * length, :] = acc.astype(jnp.bfloat16)
    gather_start(conv_slot, conv_sems)
    slot("c0")
    gather_finish(
        conv_slot, lambda j: conv_s.at[pl.ds(j * n_fs, n_fs)], conv_sems, "c"
    )
    small_copy(gain_s.at[other], gain_s.at[other], 0).wait_recv()
    small_copy(proj_s.at[other], proj_s.at[other], 1).wait_recv()

    for j in range(n_fs * n_tp // 2):
        left = conv_s[2 * j].astype(jnp.float32)
        right = conv_s[2 * j + 1].astype(jnp.float32)
        cols = slice(j * LANES, (j + 1) * LANES)
        norm_s[:top, cols] = jnp.concatenate((left[:, :chans], right[:, :chans]), axis=1)
        norm_s[top:, cols] = jnp.concatenate((left[:, chans:], right[:, chans:]), axis=1)
    gains = jnp.concatenate([gain_s[j] for j in range(n_tp)], axis=1)

    @pl.loop(0, n_fs)
    def _(i):
        here = rows_of(i)
        v = normed(norm_s[here, :]) * gains
        act_s[here, :] = (v / (1.0 + jnp.exp(-v))).astype(jnp.bfloat16)

    slot("n0")
    share = proj_s.shape[1]
    mixed_slot = lambda i, j: mixed_s.at[j * n_fs + i]
    mixed_s[t * n_fs + f] = sum(
        jnp.dot(
            act_s[:, j * share : (j + 1) * share],
            proj_s[j],
            preferred_element_type=jnp.float32,
        )
        for j in range(n_tp)
    ).astype(jnp.bfloat16)
    gather_start(mixed_slot, mixed_sems)
    slot("m0")
    gather_finish(
        mixed_slot, lambda j: mixed_s.at[pl.ds(j * n_fs, n_fs)], mixed_sems, "m"
    )
    slot("m8")

    @pl.loop(0, n_fs)
    def _(i):
        here = rows_of(i)
        skip = jnp.concatenate([x_s[j, here, :] for j in range(n_tp)], axis=1)
        added = jnp.concatenate(
            [mixed_s[j * n_fs + k, here, :] for k in range(n_fs) for j in range(n_tp)], axis=1
        )
        before = residual_scale * skip.astype(jnp.float32) + added.astype(jnp.float32)
        mid_s[here, :] = (normed(before) * mix_gain[...]).astype(jnp.bfloat16)

    slot("e0")
    near_side = hi // (n_hi // 2)
    deep = n_fs // n_tp * depth

    def partial_ff(side):
        inner_rows = pl.ds(pl.multiple_of(side * deep, deep), deep)
        left = mid_s[:, inner_rows]
        return tuple(
            jnp.dot(left, right[inner_rows, :], preferred_element_type=jnp.float32)
            for right in (gate_s, up_s)
        )

    for which in (0, 1):
        sized(f, lambda size: own_copy(which, size).wait())
        weight_finish(which, NEAR)
        slot("w" + str(which))
    ff_s[0], ff_s[1] = partial_ff(near_side)
    slot("w2")
    for i, (which, ks) in enumerate(((0, FIRST), (1, FIRST), (0, CROSS), (1, CROSS))):
        weight_finish(which, ks)
        slot("w" + str(3 + i))

    gate, upward = partial_ff(1 - near_side)
    gate, upward = gate + ff_s[0], upward + ff_s[1]
    hid_s[...] = (gate / (1.0 + jnp.exp(-gate)) * upward).astype(jnp.bfloat16)
    slot("g0")

    sized(f, lambda size: own_copy(2, size).wait())
    weight_finish(2, NEAR)
    slot("g2")
    span = down_s.shape[2]
    per_core = n_fs // n_tp
    steps = (3, 2, 1, 0)

    def project(side):
        @pl.loop(0, per_core)
        def _(j):
            part_s[side, :, pl.ds(pl.multiple_of(j * span, span), span)] = jnp.dot(
                hid_s[...], down_s[side * per_core + j], preferred_element_type=jnp.float32
            ).astype(jnp.bfloat16)

    def half_copy(k):
        here = rows_of(along(k))
        return remote(
            part_s.at[other, here],
            half_s.at[here],
            half_sems.at[0],
            half_sems.at[1 + code(k)],
            partner,
        )

    def hand_over():
        for low in (1, 0):
            for d in steps:
                half_copy((d, low)).start()

    def joined(k):
        here = rows_of(along(k))
        receive(half_s.at[here], half_sems, code(k))
        return part_s[t, here, :].astype(jnp.float32) + half_s[here, :].astype(jnp.float32)

    def aside_copy(d):
        return remote(
            sum_s.at[rows_of(along((d, 1)))], y_s.at[d], y_sems.at[0], y_sems.at[1 + d], beside
        )

    def aside():
        for d in steps:
            sum_s[rows_of(along((d, 1))), :] = joined((d, 1)).astype(jnp.bfloat16)
            aside_copy(d).start()

    project(near_side)
    pl.when(t == near_side)(aside)
    pl.when(t != near_side)(hand_over)
    slot("g3")
    weight_finish(2, FIRST + CROSS)
    project(1 - near_side)
    pl.when(t == near_side)(hand_over)
    pl.when(t != near_side)(aside)

    for d in steps:
        here = rows_of(along((d, 0)))
        forward = joined((d, 0))
        receive(y_s.at[d], y_sems, d)
        forward = forward + y_s[d].astype(jnp.float32)
        if d % 2:
            sum_s[here, :] = forward.astype(jnp.bfloat16)
            send(sum_s.at[here], z_s.at[d // 2], z_sems, d // 2, close)
        elif d:
            receive(z_s.at[1], z_sems, 1)
            sum_s[here, :] = (forward + z_s[1].astype(jnp.float32)).astype(jnp.bfloat16)
            send(sum_s.at[here], z_s.at[2], z_sems, 2, far)
    for i in (0, 2):
        receive(z_s.at[i], z_sems, i)
        forward = forward + z_s[i].astype(jnp.float32)
    forward = forward.astype(jnp.bfloat16).astype(jnp.float32)
    own_half = pl.ds(pl.multiple_of(t * feat, feat), feat)
    final = residual_scale * mid_s[rows_of(f), own_half].astype(jnp.float32) + forward
    lane = lax.broadcasted_iota(jnp.int32, (length, LANES), 1)
    stat_s[t] = jnp.where(
        lane == 0,
        jnp.sum(final, axis=1, keepdims=True),
        jnp.sum(final * final, axis=1, keepdims=True),
    )
    small_copy(stat_s.at[t], stat_s.at[t], 2).start()
    small_copy(stat_s.at[other], stat_s.at[other], 2).wait_recv()
    stats = (stat_s[0] + stat_s[1]) / model
    average, second = stats[:, 0:1], stats[:, 1:2]
    scaled = (final - average) * lax.rsqrt(second - average * average + epsilon)
    out_s[...] = (scaled * out_gain[t]).astype(jnp.bfloat16)
    result = pltpu.make_async_copy(out_s, out.at[0], local_sems.at[7])
    result.start()
    result.wait()
    blocks = n_fs * n_tp - 1
    sent(mixed_s.at[pl.ds(0, blocks)], tok_sems.at[0])
    sent(conv_s.at[pl.ds(0, blocks)], conv_sems.at[0])
    sent(mixed_s.at[pl.ds(0, blocks)], mixed_sems.at[0])
    sent(seven, glu_sems.at[0])
    sent(seven, glu_cross_sems.at[0])
    sent(half_s, half_sems.at[0])
    sent(y_s, y_sems.at[0])
    sent(z_s, z_sems.at[0])
    small_copy(gain, gain_s.at[t], 0).wait_send()
    small_copy(out_weight.at[:, columns], proj_s.at[t], 1).wait_send()
    small_copy(stat_s.at[t], stat_s.at[t], 2).wait_send()
    for k in OTHERS:
        deep_rows = pl.ds(0, (4 if k in NEAR else 3) * half_depth)
        sized(
            along(k),
            lambda size: sent(
                gate_s.at[deep_rows, pl.ds(0, size)], ff_sems.at[3 * n_fs + code(k)]
            ),
        )
    for i, count in enumerate((2 * len(OTHERS), len(FIRST + CROSS))):
        sized(
            f,
            lambda size: sent(
                gate_s.at[pl.ds(0, count * half_depth), pl.ds(0, size)], cross_sems.at[i]
            ),
        )


def by_kernel(
    tokens,
    lin_weight,
    glu_weight,
    conv_taps,
    conv_gain,
    conv_out_weight,
    mix_gain,
    ff_gate,
    ff_up,
    ff_down,
    out_gain,
):
    n_fs, n_tp = lax.axis_size("fs"), lax.axis_size("tp")
    _, length, feat = tokens.shape
    rows, model = n_fs * length, feat * n_tp
    depth, own_chans = lin_weight.shape
    chans = own_chans // n_fs
    width, narrow = widths(ff_gate.shape[1], n_fs)
    vmem, far = pl.BlockSpec(memory_space=pltpu.VMEM), pl.BlockSpec(memory_space=pl.ANY)
    bf, fl = jnp.bfloat16, jnp.float32
    span = ff_down.shape[1]
    dma = lambda n: pltpu.SemaphoreType.DMA((n,))
    result = pl.pallas_call(
        functools.partial(fused, n_fs, n_tp, width, narrow),
        out_shape=jax.ShapeDtypeStruct((1, length, feat), bf),
        in_specs=[far] * 4 + [vmem] * 3 + [far] * 3 + [vmem],
        out_specs=far,
        scratch_shapes=[
            pltpu.VMEM((n_tp, rows, feat), bf),
            pltpu.VMEM((depth, own_chans), bf),
            pltpu.VMEM((depth, own_chans), bf),
            pltpu.VMEM(conv_taps.shape, fl),
            pltpu.VMEM((n_fs, depth, 2 * chans), bf),
            pltpu.VMEM((n_fs * depth, 2 * chans), bf),
            pltpu.VMEM((n_tp, 1, own_chans), fl),
            pltpu.VMEM((n_tp, own_chans, span // n_tp), bf),
            pltpu.VMEM((n_fs // 2, length + 32, LANES), fl),
            pltpu.VMEM((n_fs * n_tp, rows // 2, LANES), bf),
            pltpu.VMEM((rows, own_chans * n_tp), fl),
            pltpu.VMEM((rows, own_chans * n_tp), bf),
            pltpu.VMEM((n_fs * n_tp, rows, LANES), bf),
            pltpu.VMEM((rows, model), bf),
            pltpu.VMEM((n_fs * depth, width), bf),
            pltpu.VMEM((n_fs * depth, width), bf),
            pltpu.VMEM((n_fs, width, span), bf),
            pltpu.VMEM((2, rows, width), fl),
            pltpu.VMEM((rows, width), bf),
            pltpu.VMEM((n_tp, rows, feat), bf),
            pltpu.VMEM((rows, feat), bf),
            pltpu.VMEM((rows, feat), bf),
            pltpu.VMEM((3, length, feat), bf),
            pltpu.VMEM((n_fs // 2, length, feat), bf),
            pltpu.VMEM((n_tp, length, LANES), fl),
            pltpu.VMEM((length, feat), bf),
            dma(n_fs + 1),
            dma(2),
            dma(6),
            dma(n_fs + 1),
            dma(n_fs + 1),
            dma(n_fs + 1),
            dma(4 * n_fs),
            dma(9),
            dma(8),
            dma(n_fs + 1),
            dma(4),
            dma(n_fs // 2 + 1),
        ],
        compiler_params=pltpu.CompilerParams(
            collective_id=0, has_side_effects=True, vmem_limit_bytes=60 * 2**20
        ),
    )(
        tokens[0],
        lin_weight,
        glu_weight,
        conv_taps,
        conv_gain[None],
        conv_out_weight,
        mix_gain[None],
        ff_gate,
        ff_up,
        ff_down,
        out_gain.reshape(n_tp, 1, feat),
    )
    return result


def widths(units, n_fs):
    half = n_fs // 2
    blocks = units // LANES // 2
    most = -(-blocks // half)
    return most * LANES, (blocks - most * (half - 1)) * LANES


def on_device(*args):
    tokens, lin_weight, conv_out_weight, ff_gate = args[0], args[1], args[5], args[7]
    n_fs, n_tp, n_rep = (lax.axis_size(a) for a in ("fs", "tp", "rep"))
    seqs, length, feat = tokens.shape
    units = ff_gate.shape[1]
    width, narrow = widths(units, n_fs)
    fits = (
        n_rep == 2
        and n_tp == 2
        and n_fs == 8
        and seqs == 1
        and length % 16 == 0
        and args[3].shape[0] <= 33
        and lin_weight.shape[1] * 2 == n_fs * LANES
        and conv_out_weight.shape[1] == n_tp * LANES
        and feat % LANES == 0
        and units % (2 * LANES) == 0
        and narrow == width - LANES > 0
        and lin_weight.shape[0] % 32 == 0
    )
    if fits:
        return by_kernel(*args)
    return by_collectives(*args)


def solution(mesh):
    mapped = jax.shard_map(
        on_device,
        mesh=mesh,
        in_specs=(
            P(("rep", "fs"), None, "tp"),
            P("fs", "tp"),
            P("fs", "tp"),
            P(None, "tp"),
            P("tp"),
            P("tp", "fs"),
            P(),
            P("fs", "tp"),
            P("fs", "tp"),
            P("tp", "fs"),
            P(),
        ),
        out_specs=P(("rep", "fs"), None, "tp"),
        check_vma=False,
    )
    return mapped
```

```python
import functools

import jax
import jax.numpy as jnp
from jax import lax
from jax.experimental import pallas as pl
from jax.experimental.pallas import tpu as pltpu
from jax.sharding import PartitionSpec as P

residual_scale = 2.0**0.25
epsilon = 1e-05


def normed(values):
    average = jnp.mean(values, axis=-1, keepdims=True)
    second = jnp.mean(values * values, axis=-1, keepdims=True)
    return (values - average) * lax.rsqrt(second - average * average + epsilon)


def interleave(left, right, parts):
    rows, width = left.shape
    pair = jnp.concatenate(
        (left.reshape(rows, parts, width // parts), right.reshape(rows, parts, width // parts)),
        axis=2,
    )
    return pair.reshape(rows, 2 * width)


def by_collectives(
    tokens,
    lin_weight,
    glu_weight,
    conv_taps,
    conv_gain,
    conv_out_weight,
    mix_gain,
    ff_gate,
    ff_up,
    ff_down,
    out_gain,
):
    n_fs, n_tp = lax.axis_size("fs"), lax.axis_size("tp")
    fs_index, tp_index = lax.axis_index("fs"), lax.axis_index("tp")
    seqs, length, feat = tokens.shape
    groups = n_fs * seqs
    rows = groups * length
    model = feat * n_tp
    conv_gain_all = lax.all_gather(conv_gain, "tp", axis=0, tiled=True)

    gathered = lax.all_gather(tokens, ("fs", "tp"), axis=0, tiled=False)
    all_tokens = (
        gathered.reshape(n_fs, n_tp, seqs, length, feat)
        .transpose(0, 2, 3, 1, 4)
        .reshape(rows, model)
    )
    glu_pair = lax.all_to_all(
        interleave(lin_weight, glu_weight, n_fs), "fs", split_axis=1, concat_axis=0, tiled=True
    )
    own_out = lax.all_to_all(conv_out_weight, "tp", split_axis=1, concat_axis=0, tiled=True)
    ff_pair = lax.all_to_all(
        interleave(ff_gate, ff_up, n_fs), "fs", split_axis=1, concat_axis=0, tiled=True
    )
    own_down = lax.all_to_all(ff_down, "fs", split_axis=0, concat_axis=1, tiled=True)

    chans = glu_pair.shape[1] // 2
    product = jnp.dot(all_tokens, glu_pair, preferred_element_type=jnp.float32)
    glu = (product[:, :chans] * jax.nn.sigmoid(product[:, chans:])).astype(jnp.bfloat16)
    n_taps = conv_taps.shape[0]
    margin = (n_taps - 1) // 2
    own_taps = lax.dynamic_slice_in_dim(conv_taps, fs_index * chans, chans, 1)
    padded = jnp.pad(
        glu.astype(jnp.float32).reshape(groups, length, chans),
        ((0, 0), (margin, margin), (0, 0)),
    )
    conv = sum(padded[:, k : k + length] * own_taps[k] for k in range(n_taps))
    conv = conv.reshape(rows, chans).astype(jnp.bfloat16)
    conv_all = lax.all_gather(conv, ("tp", "fs"), axis=1, tiled=True)
    activated = jax.nn.silu(normed(conv_all.astype(jnp.float32)) * conv_gain_all).astype(
        jnp.bfloat16
    )
    mixed_own = jnp.dot(activated, own_out, preferred_element_type=jnp.float32).astype(
        jnp.bfloat16
    )
    mixed = lax.all_gather(mixed_own, ("fs", "tp"), axis=1, tiled=True)
    before = residual_scale * all_tokens.astype(jnp.float32) + mixed.astype(jnp.float32)
    middle = (normed(before) * mix_gain).astype(jnp.bfloat16)

    units = ff_pair.shape[1] // 2
    both = jnp.dot(middle, ff_pair, preferred_element_type=jnp.float32)
    hidden = (jax.nn.silu(both[:, :units]) * both[:, units:]).astype(jnp.bfloat16)
    down = jnp.dot(hidden, own_down, preferred_element_type=jnp.float32).astype(jnp.bfloat16)
    sends = (
        down.reshape(n_fs, seqs * length, n_tp, feat)
        .transpose(0, 2, 1, 3)
        .reshape(n_fs * n_tp, seqs * length, feat)
    )
    arrived = lax.all_to_all(sends, ("fs", "tp"), split_axis=0, concat_axis=0, tiled=True)
    forward = jnp.sum(arrived.astype(jnp.float32), axis=0)
    forward = forward.astype(jnp.bfloat16).astype(jnp.float32)
    middle_own = lax.dynamic_slice(
        middle,
        (fs_index * seqs * length, tp_index * feat),
        (seqs * length, feat),
    )
    final = residual_scale * middle_own.astype(jnp.float32) + forward
    sums, squares = lax.psum(
        (jnp.sum(final, axis=1, keepdims=True), jnp.sum(final * final, axis=1, keepdims=True)),
        "tp",
    )
    average = sums / model
    out = (final - average) * lax.rsqrt(squares / model - average * average + epsilon)
    gain = lax.dynamic_slice_in_dim(out_gain, tp_index * feat, feat, 0)
    return (out * gain).astype(jnp.bfloat16).reshape(seqs, length, feat)


MESH = pl.DeviceIdType.MESH
LANES = 128
FIRST = ((2, 0), (3, 0))
CROSS = ((2, 1), (3, 1))
NEAR = ((1, 0), (1, 1), (0, 1))
OTHERS = FIRST + CROSS + NEAR
G, U, D = 0, 1, 2
INNER = {
    "t0": ((1, G, 2, 0), (1, G, 3, 0), (1, G, 0, 1),),
    "t3": ((1, U, 2, 0),),
    "t5": ((1, U, 3, 0), (1, G, 1, 0),),
    "t6": ((1, G, 1, 1),),
    "t7": ((1, G, 2, 1), (1, D, 0, 1),),
    "c0": ((1, G, 3, 1),),
    "c2": ((0, G, 3, 0), (1, U, 1, 0),),
    "c3": ((1, U, 2, 1), (1, U, 3, 1),),
    "c4": ((0, G, 2, 0), (0, U, 3, 0), (1, U, 1, 1),),
    "c6": ((0, G, 1, 0), (0, U, 2, 0),),
    "c7": ((1, U, 0, 1), (1, D, 2, 0), (0, G, 0, 1),),
    "m0": ((1, D, 3, 0), (0, G, 3, 1), (0, G, 2, 1),),
    "m1": ((0, U, 3, 1), (0, U, 2, 1),),
    "m2": ((0, U, 1, 0), (0, U, 0, 1),),
    "m3": ((0, G, 1, 1),),
    "m4": ((1, D, 1, 0), (0, U, 1, 1),),
    "m5": ((1, D, 2, 1), (1, D, 3, 1), (1, D, 1, 1),),
    "m6": ((0, D, 2, 0),),
    "m7": ((0, D, 3, 0),),
    "w2": ((0, D, 3, 1), (0, D, 2, 1),),
}
OUTER = {
    "t3": ((1, G, 2, 0), (1, G, 3, 0),),
    "t5": ((1, U, 2, 0), (1, G, 1, 0),),
    "t7": ((1, D, 0, 1),),
    "c0": ((1, U, 3, 0),),
    "c2": ((0, G, 2, 0),),
    "c3": ((1, G, 2, 1), (1, G, 3, 1),),
    "c4": ((0, U, 2, 0), (0, G, 3, 0), (0, G, 1, 0),),
    "c5": ((1, U, 2, 1), (1, U, 3, 1),),
    "c6": ((0, U, 3, 0), (0, G, 1, 1),),
    "c7": ((1, U, 0, 1), (1, U, 1, 0), (1, G, 1, 1), (0, G, 0, 1),),
    "m0": ((1, U, 1, 1), (0, G, 2, 1), (0, G, 3, 1),),
    "m1": ((0, U, 2, 1),),
    "m2": ((0, U, 3, 1),),
    "m3": ((1, D, 2, 0), (0, U, 1, 0), (0, U, 0, 1),),
    "m4": ((0, U, 1, 1),),
    "m5": ((1, D, 3, 0), (1, D, 2, 1), (1, D, 3, 1),),
    "m7": ((0, D, 2, 0), (1, D, 1, 0), (1, D, 1, 1),),
    "m8": ((0, D, 3, 0),),
    "w2": ((0, D, 3, 1), (0, D, 2, 1),),
    "t0": ((1, G, 0, 1),),
}

def fused(
    n_fs,
    n_tp,
    width,
    narrow,
    tok,
    lin_hbm,
    glu_hbm,
    taps_hbm,
    gain,
    out_weight,
    mix_gain,
    gate_hbm,
    up_hbm,
    down_hbm,
    out_gain,
    out,
    x_s,
    lin_s,
    gl_s,
    taps_s,
    mix_s,
    glu_s,
    gain_s,
    proj_s,
    pad_s,
    conv_s,
    norm_s,
    act_s,
    mixed_s,
    mid_s,
    gate_s,
    up_s,
    down_s,
    ff_s,
    hid_s,
    part_s,
    half_s,
    sum_s,
    z_s,
    y_s,
    stat_s,
    out_s,
    glu_sems,
    glu_cross_sems,
    small_sems,
    tok_sems,
    conv_sems,
    mixed_sems,
    ff_sems,
    cross_sems,
    local_sems,
    half_sems,
    z_sems,
    y_sems,
):
    rep, f, t = lax.axis_index("rep"), lax.axis_index("fs"), lax.axis_index("tp")
    other = 1 - t
    n_hi = n_fs // 2
    hi, lo = f // 2, f % 2
    rows, feat = x_s.shape[1:]
    length = rows // n_fs
    model = feat * n_tp
    depth = gate_hbm.shape[0]
    half_depth = depth // 2
    chans = LANES // 2

    def flip(z, step):
        return z + step - 2 * step * ((z // step) % 2)

    def along(k):
        z = hi
        for step in (1, 2):
            if k[0] & step:
                z = flip(z, step)
        return z * 2 + (1 - lo if k[1] else lo)

    def code(k):
        return k[0] * 2 + k[1]

    barrier = pltpu.get_barrier_semaphore()
    for k in OTHERS:
        pl.semaphore_signal(barrier, inc=1, device_id=(rep, along(k), t), device_id_type=MESH)
    pl.semaphore_signal(barrier, inc=1, device_id=(rep, f, other), device_id_type=MESH)
    pl.semaphore_signal(barrier, inc=1, device_id=(1 - rep, f, t), device_id_type=MESH)

    def rows_of(i):
        return pl.ds(pl.multiple_of(i * length, length), length)

    def depth_of(i, part, size):
        return pl.ds(pl.multiple_of(i * depth + part * half_depth, half_depth), size)

    def tok_slot(i, j):
        return x_s.at[j, rows_of(i)]

    per_half = n_fs // 2

    def start_of(i):
        return pl.multiple_of((i * (width // LANES) - i // per_half) * LANES, LANES)

    def is_short(i):
        return i % per_half == per_half - 1

    def sized(i, action):
        @pl.when(jnp.logical_not(is_short(i)))
        def _():
            action(width)

        @pl.when(is_short(i))
        def _():
            action(narrow)

    fetches = [
        pltpu.make_async_copy(src, dst, local_sems.at[n])
        for n, (src, dst) in enumerate(
            (
                (tok, tok_slot(f, t)),
                (lin_hbm, lin_s),
                (glu_hbm, gl_s),
                (taps_hbm, taps_s),
            )
        )
    ]
    for copy in fetches:
        copy.start()

    def own_copy(which, size):
        first = start_of(f)
        src, dst = (
            (gate_hbm.at[:, pl.ds(first, size)], gate_s.at[depth_of(f, 0, depth), pl.ds(0, size)]),
            (up_hbm.at[:, pl.ds(first, size)], up_s.at[depth_of(f, 0, depth), pl.ds(0, size)]),
            (down_hbm.at[pl.ds(first, size)], down_s.at[f, pl.ds(0, size)]),
        )[which]
        return pltpu.make_async_copy(src, dst, local_sems.at[4 + which])

    for which in range(3):
        sized(f, lambda size, which=which: own_copy(which, size).start())

    @pl.when(is_short(f))
    def _():
        gate_s[:, narrow:] = jnp.zeros((n_fs * depth, width - narrow), jnp.bfloat16)
        up_s[:, narrow:] = jnp.zeros((n_fs * depth, width - narrow), jnp.bfloat16)
        down_s[:, narrow:, :] = jnp.zeros((n_fs, width - narrow, down_s.shape[2]), jnp.bfloat16)

    def remote(src, dst, send_sem, recv_sem, device):
        return pltpu.make_async_remote_copy(
            src_ref=src,
            dst_ref=dst,
            send_sem=send_sem,
            recv_sem=recv_sem,
            device_id=device,
            device_id_type=MESH,
        )

    def send(src, dst, sems, index, device):
        remote(src, dst, sems.at[0], sems.at[1 + index], device).start()

    partner = (rep, f, other)
    mirror = (1 - rep, f, t)
    beside = (rep, along((0, 1)), t)
    close = (rep, along((1, 0)), t)
    far = (rep, along((2, 0)), t)

    def arrive(dst, sem):
        remote(dst, dst, sem, sem, partner).wait_recv()

    def receive(dst, sems, index):
        arrive(dst, sems.at[1 + index])

    def sent(src, sem):
        remote(src, src, sem, sem, partner).wait_send()

    def small_copy(src, dst, index):
        return remote(src, dst, small_sems.at[index], small_sems.at[3 + index], partner)

    def gather_start(slot, sems):
        block = slot(f, t)
        send(block, block, sems, 0, far)
        send(block, block, sems, 1, close)
        send(block, block, sems, 3, beside)
        send(block, block, sems, 7, partner)

    inner = (hi % n_hi) // (n_hi // 2) != hi % 2

    def slot(name):
        for role, table in ((inner, INNER), (jnp.logical_not(inner), OUTER)):
            steps = table.get(name, ())

            @pl.when(role)
            def _(steps=steps):
                for send_it, which, *k in steps:
                    (weight_send if send_it else weight_forward)(which, tuple(k))

    def gather_finish(place, all_of, sems, name, between=None):
        between = between or {}

        def pause(step):
            slot(name + str(step))
            if step in between:
                between[step]()

        def got(index, k):
            block = place(along(k), t)
            receive(block, sems, index)
            return block

        block = got(3, (0, 1))
        send(block, block, sems, 7, partner)
        pause(1)
        block = got(0, (2, 0))
        send(block, block, sems, 2, close)
        send(block, block, sems, 5, beside)
        send(block, block, sems, 7, partner)
        pause(2)
        block = got(1, (1, 0))
        send(block, block, sems, 4, beside)
        send(block, block, sems, 7, partner)
        pause(3)
        block = got(4, (1, 1))
        send(block, block, sems, 7, partner)
        pause(4)
        block = got(2, (3, 0))
        send(block, block, sems, 6, beside)
        send(block, block, sems, 7, partner)
        pause(5)
        block = got(5, (2, 1))
        send(block, block, sems, 7, partner)
        pause(6)
        block = got(6, (3, 1))
        send(block, block, sems, 7, partner)
        pause(7)
        receive(all_of(other), sems, 7)

    half_width = width // 2

    def piece(which, to, source, part, size):
        first = start_of(to)
        ups = pl.ds(pl.multiple_of(part * half_depth, half_depth), half_depth)
        spot = depth_of(source, part, half_depth)
        deep = pl.ds(pl.multiple_of(part * (size // 2), size // 2), size // 2)
        from_down = pl.ds(pl.multiple_of(first + part * (size // 2), LANES // 2), size // 2)
        return (
            (gate_hbm.at[ups, pl.ds(first, size)], gate_s.at[spot, pl.ds(0, size)]),
            (up_hbm.at[ups, pl.ds(first, size)], up_s.at[spot, pl.ds(0, size)]),
            (down_hbm.at[from_down], down_s.at[source, deep]),
        )[which]

    def whole(which, k):
        return which == D and k in NEAR

    def weight_copy(which, k, size):
        to = along(k)
        if whole(which, k):
            src, dst = down_hbm.at[pl.ds(start_of(to), size)], down_s.at[f, pl.ds(0, size)]
        else:
            src, dst = piece(which, to, f, rep, size)
        return remote(
            src, dst, ff_sems.at[3 * n_fs + code(k)], ff_sems.at[which * n_fs + code(k)], (rep, to, t)
        )

    def weight_send(which, k):
        sized(along(k), lambda size: weight_copy(which, k, size).start())

    def group_sem(which, k):
        group = 0 if k in NEAR else 1 if k in FIRST else 2
        return cross_sems.at[2 + (6 if which == D else 3 * which + group)]

    def cross_copy(which, k, size):
        block = piece(which, f, along(k), rep, size)[1]
        return remote(block, block, cross_sems.at[which // 2], group_sem(which, k), mirror)

    def weight_forward(which, k):
        def action(size):
            block = piece(which, f, along(k), rep, size)[1]
            arrive(block, ff_sems.at[which * n_fs + code(k)])
            cross_copy(which, k, size).start()

        sized(f, action)

    def weight_finish(which, ks):
        def action(size):
            if whole(which, ks[0]):
                for k in ks:
                    arrive(down_s.at[along(k), pl.ds(0, size)], ff_sems.at[which * n_fs + code(k)])
            else:
                arrive(
                    gate_s.at[pl.ds(0, len(ks) * half_depth), pl.ds(0, size)],
                    group_sem(which, ks[0]),
                )

        sized(f, action)

    pl.semaphore_wait(barrier, n_fs + 1)
    fetches[0].wait()
    gather_start(tok_slot, tok_sems)
    fetches[1].wait()
    fetches[2].wait()
    for d in range(n_fs):
        cols = slice(d * chans, (d + 1) * chans)
        mix_s[d] = jnp.concatenate((lin_s[:, cols], gl_s[:, cols]), axis=1)

    def glu_piece(source, part):
        return glu_s.at[depth_of(source, part, half_depth)]

    for k in OTHERS:
        to = along(k)
        own_rows = pl.ds(pl.multiple_of(rep * half_depth, half_depth), half_depth)
        send(mix_s.at[to, own_rows], glu_piece(f, rep), glu_sems, code(k), (rep, to, t))
    slot("t0")
    columns = pl.ds(pl.multiple_of(other * LANES, LANES), LANES)
    own_columns = pl.ds(pl.multiple_of(t * LANES, LANES), LANES)
    small_copy(gain, gain_s.at[t], 0).start()
    small_copy(out_weight.at[:, columns], proj_s.at[t], 1).start()

    glu_s[pl.ds(pl.multiple_of(f * depth, depth), depth), :] = mix_s[f]
    gain_s[t] = gain[...]
    proj_s[t] = out_weight[:, own_columns]
    pad_s[...] = jnp.zeros_like(pad_s)

    def glu_forward(ks):
        for k in ks:
            block = glu_piece(along(k), rep)
            receive(block, glu_sems, code(k))
            send(block, block, glu_cross_sems, 0, mirror)

    gather_finish(
        tok_slot,
        lambda j: x_s.at[j],
        tok_sems,
        "t",
        {
            4: lambda: glu_forward(NEAR),
            5: lambda: glu_forward(FIRST),
            6: lambda: glu_forward(CROSS),
        },
    )
    seven = glu_s.at[pl.ds(0, len(OTHERS) * half_depth)]
    receive(seven, glu_cross_sems, 0)

    product = sum(
        jnp.dot(
            x_s[j], glu_s[j * feat : (j + 1) * feat], preferred_element_type=jnp.float32
        )
        for j in range(n_tp)
    )
    glu = product[:, :chans] / (1.0 + jnp.exp(-product[:, chans:]))
    top = rows // 2
    packed = jnp.concatenate((glu[:top], glu[top:]), axis=1)
    packed = packed.astype(jnp.bfloat16).astype(jnp.float32)
    fetches[3].wait()
    lanes = lax.broadcasted_iota(jnp.int32, (1, LANES), 1)
    tap_pair = taps_s[:, pl.ds(pl.multiple_of(f // 2 * LANES, LANES), LANES)]
    turned = pltpu.roll(tap_pair, chans, 1)
    taps = jnp.where((lanes < chans) == (f % 2 == 0), tap_pair, turned)
    n_taps = taps.shape[0]
    margin = (n_taps - 1) // 2
    slot("d0")
    conv_slot = lambda i, j: conv_s.at[j * n_fs + i]
    groups = n_fs // 2
    for g in range(groups):
        pad_s[g, 16 : 16 + length, :] = packed[g * length : (g + 1) * length]
    for g in range(groups):
        acc = jnp.zeros((length, LANES), jnp.float32)
        for k in range(n_taps):
            first = 16 - margin + k
            acc = acc + pad_s[g, first : first + length, :] * taps[k : k + 1, :]
        conv_s[t * n_fs + f, g * length : (g + 1) * length, :] = acc.astype(jnp.bfloat16)
    gather_start(conv_slot, conv_sems)
    slot("c0")
    gather_finish(
        conv_slot, lambda j: conv_s.at[pl.ds(j * n_fs, n_fs)], conv_sems, "c"
    )
    small_copy(gain_s.at[other], gain_s.at[other], 0).wait_recv()
    small_copy(proj_s.at[other], proj_s.at[other], 1).wait_recv()

    for j in range(n_fs * n_tp // 2):
        left = conv_s[2 * j].astype(jnp.float32)
        right = conv_s[2 * j + 1].astype(jnp.float32)
        cols = slice(j * LANES, (j + 1) * LANES)
        norm_s[:top, cols] = jnp.concatenate((left[:, :chans], right[:, :chans]), axis=1)
        norm_s[top:, cols] = jnp.concatenate((left[:, chans:], right[:, chans:]), axis=1)
    gains = jnp.concatenate([gain_s[j] for j in range(n_tp)], axis=1)

    @pl.loop(0, n_fs)
    def _(i):
        here = rows_of(i)
        v = normed(norm_s[here, :]) * gains
        act_s[here, :] = (v / (1.0 + jnp.exp(-v))).astype(jnp.bfloat16)

    slot("n0")
    share = proj_s.shape[1]
    mixed_slot = lambda i, j: mixed_s.at[j * n_fs + i]
    mixed_s[t * n_fs + f] = sum(
        jnp.dot(
            act_s[:, j * share : (j + 1) * share],
            proj_s[j],
            preferred_element_type=jnp.float32,
        )
        for j in range(n_tp)
    ).astype(jnp.bfloat16)
    gather_start(mixed_slot, mixed_sems)
    slot("m0")
    gather_finish(
        mixed_slot, lambda j: mixed_s.at[pl.ds(j * n_fs, n_fs)], mixed_sems, "m"
    )
    slot("m8")

    @pl.loop(0, n_fs)
    def _(i):
        here = rows_of(i)
        skip = jnp.concatenate([x_s[j, here, :] for j in range(n_tp)], axis=1)
        added = jnp.concatenate(
            [mixed_s[j * n_fs + k, here, :] for k in range(n_fs) for j in range(n_tp)], axis=1
        )
        before = residual_scale * skip.astype(jnp.float32) + added.astype(jnp.float32)
        mid_s[here, :] = (normed(before) * mix_gain[...]).astype(jnp.bfloat16)

    slot("e0")
    near_side = hi // (n_hi // 2)
    deep = n_fs // n_tp * depth

    def partial_ff(side):
        inner_rows = pl.ds(pl.multiple_of(side * deep, deep), deep)
        left = mid_s[:, inner_rows]
        return tuple(
            jnp.dot(left, right[inner_rows, :], preferred_element_type=jnp.float32)
            for right in (gate_s, up_s)
        )

    for which in (0, 1):
        sized(f, lambda size: own_copy(which, size).wait())
        weight_finish(which, NEAR)
        slot("w" + str(which))
    ff_s[0], ff_s[1] = partial_ff(near_side)
    slot("w2")
    for i, (which, ks) in enumerate(((0, FIRST), (1, FIRST), (0, CROSS), (1, CROSS))):
        weight_finish(which, ks)
        slot("w" + str(3 + i))

    gate, upward = partial_ff(1 - near_side)
    gate, upward = gate + ff_s[0], upward + ff_s[1]
    hid_s[...] = (gate / (1.0 + jnp.exp(-gate)) * upward).astype(jnp.bfloat16)
    slot("g0")

    sized(f, lambda size: own_copy(2, size).wait())
    weight_finish(2, NEAR)
    slot("g2")
    span = down_s.shape[2]
    per_core = n_fs // n_tp
    steps = (3, 2, 1, 0)

    def project(side):
        @pl.loop(0, per_core)
        def _(j):
            part_s[side, :, pl.ds(pl.multiple_of(j * span, span), span)] = jnp.dot(
                hid_s[...], down_s[side * per_core + j], preferred_element_type=jnp.float32
            ).astype(jnp.bfloat16)

    pieces_of = tuple((d, h) for d in steps for h in (0, 1))

    def cols(h):
        return pl.ds(h * (feat // 2), feat // 2)

    def half_copy(k, h):
        here = rows_of(along(k))
        return remote(
            part_s.at[other, here, cols(h)],
            half_s.at[here, cols(h)],
            half_sems.at[0],
            half_sems.at[1 + 2 * code(k) + h],
            partner,
        )

    def hand_over():
        for low in (1, 0):
            for d, h in pieces_of:
                half_copy((d, low), h).start()

    def joined(k, h):
        here = rows_of(along(k))
        receive(half_s.at[here, cols(h)], half_sems, 2 * code(k) + h)
        return part_s[t, here, cols(h)].astype(jnp.float32) + half_s[here, cols(h)].astype(
            jnp.float32
        )

    def aside_copy(d, h):
        return remote(
            sum_s.at[rows_of(along((d, 1))), cols(h)],
            y_s.at[d, :, cols(h)],
            y_sems.at[0],
            y_sems.at[1 + 2 * d + h],
            beside,
        )

    def aside():
        for d, h in pieces_of:
            sum_s[rows_of(along((d, 1))), cols(h)] = joined((d, 1), h).astype(jnp.bfloat16)
            aside_copy(d, h).start()

    project(near_side)
    pl.when(t == near_side)(aside)
    pl.when(t != near_side)(hand_over)
    slot("g3")
    weight_finish(2, FIRST + CROSS)
    project(1 - near_side)
    pl.when(t == near_side)(hand_over)
    pl.when(t != near_side)(aside)

    def z_part(i, h):
        return z_s.at[i, :, cols(h)]

    ends = []
    for d, h in pieces_of:
        here = rows_of(along((d, 0)))
        forward = joined((d, 0), h)
        receive(y_s.at[d, :, cols(h)], y_sems, 2 * d + h)
        forward = forward + y_s[d, :, cols(h)].astype(jnp.float32)
        if d == 2:
            receive(z_part(1, h), z_sems, 2 + h)
            forward = forward + z_s[1, :, cols(h)].astype(jnp.float32)
        if d:
            sum_s[here, cols(h)] = forward.astype(jnp.bfloat16)
            slot_of = d // 2 if d % 2 else 2
            send(
                sum_s.at[here, cols(h)],
                z_part(slot_of, h),
                z_sems,
                2 * slot_of + h,
                close if d % 2 else far,
            )
        else:
            ends.append(forward)
    for i in (0, 2):
        for h in (0, 1):
            receive(z_part(i, h), z_sems, 2 * i + h)
            ends[h] = ends[h] + z_s[i, :, cols(h)].astype(jnp.float32)
    forward = jnp.concatenate(ends, axis=1)
    forward = forward.astype(jnp.bfloat16).astype(jnp.float32)
    own_half = pl.ds(pl.multiple_of(t * feat, feat), feat)
    final = residual_scale * mid_s[rows_of(f), own_half].astype(jnp.float32) + forward
    lane = lax.broadcasted_iota(jnp.int32, (length, LANES), 1)
    stat_s[t] = jnp.where(
        lane == 0,
        jnp.sum(final, axis=1, keepdims=True),
        jnp.sum(final * final, axis=1, keepdims=True),
    )
    small_copy(stat_s.at[t], stat_s.at[t], 2).start()
    small_copy(stat_s.at[other], stat_s.at[other], 2).wait_recv()
    stats = (stat_s[0] + stat_s[1]) / model
    average, second = stats[:, 0:1], stats[:, 1:2]
    scaled = (final - average) * lax.rsqrt(second - average * average + epsilon)
    out_s[...] = (scaled * out_gain[t]).astype(jnp.bfloat16)
    result = pltpu.make_async_copy(out_s, out.at[0], local_sems.at[7])
    result.start()
    result.wait()
    blocks = n_fs * n_tp - 1
    sent(mixed_s.at[pl.ds(0, blocks)], tok_sems.at[0])
    sent(conv_s.at[pl.ds(0, blocks)], conv_sems.at[0])
    sent(mixed_s.at[pl.ds(0, blocks)], mixed_sems.at[0])
    sent(seven, glu_sems.at[0])
    sent(seven, glu_cross_sems.at[0])
    sent(half_s, half_sems.at[0])
    sent(y_s, y_sems.at[0])
    sent(z_s, z_sems.at[0])
    small_copy(gain, gain_s.at[t], 0).wait_send()
    small_copy(out_weight.at[:, columns], proj_s.at[t], 1).wait_send()
    small_copy(stat_s.at[t], stat_s.at[t], 2).wait_send()
    for k in OTHERS:
        deep_rows = pl.ds(0, (4 if k in NEAR else 3) * half_depth)
        sized(
            along(k),
            lambda size: sent(
                gate_s.at[deep_rows, pl.ds(0, size)], ff_sems.at[3 * n_fs + code(k)]
            ),
        )
    for i, count in enumerate((2 * len(OTHERS), len(FIRST + CROSS))):
        sized(
            f,
            lambda size: sent(
                gate_s.at[pl.ds(0, count * half_depth), pl.ds(0, size)], cross_sems.at[i]
            ),
        )


def by_kernel(
    tokens,
    lin_weight,
    glu_weight,
    conv_taps,
    conv_gain,
    conv_out_weight,
    mix_gain,
    ff_gate,
    ff_up,
    ff_down,
    out_gain,
):
    n_fs, n_tp = lax.axis_size("fs"), lax.axis_size("tp")
    _, length, feat = tokens.shape
    rows, model = n_fs * length, feat * n_tp
    depth, own_chans = lin_weight.shape
    chans = own_chans // n_fs
    width, narrow = widths(ff_gate.shape[1], n_fs)
    vmem, far = pl.BlockSpec(memory_space=pltpu.VMEM), pl.BlockSpec(memory_space=pl.ANY)
    bf, fl = jnp.bfloat16, jnp.float32
    span = ff_down.shape[1]
    dma = lambda n: pltpu.SemaphoreType.DMA((n,))
    result = pl.pallas_call(
        functools.partial(fused, n_fs, n_tp, width, narrow),
        out_shape=jax.ShapeDtypeStruct((1, length, feat), bf),
        in_specs=[far] * 4 + [vmem] * 3 + [far] * 3 + [vmem],
        out_specs=far,
        scratch_shapes=[
            pltpu.VMEM((n_tp, rows, feat), bf),
            pltpu.VMEM((depth, own_chans), bf),
            pltpu.VMEM((depth, own_chans), bf),
            pltpu.VMEM(conv_taps.shape, fl),
            pltpu.VMEM((n_fs, depth, 2 * chans), bf),
            pltpu.VMEM((n_fs * depth, 2 * chans), bf),
            pltpu.VMEM((n_tp, 1, own_chans), fl),
            pltpu.VMEM((n_tp, own_chans, span // n_tp), bf),
            pltpu.VMEM((n_fs // 2, length + 32, LANES), fl),
            pltpu.VMEM((n_fs * n_tp, rows // 2, LANES), bf),
            pltpu.VMEM((rows, own_chans * n_tp), fl),
            pltpu.VMEM((rows, own_chans * n_tp), bf),
            pltpu.VMEM((n_fs * n_tp, rows, LANES), bf),
            pltpu.VMEM((rows, model), bf),
            pltpu.VMEM((n_fs * depth, width), bf),
            pltpu.VMEM((n_fs * depth, width), bf),
            pltpu.VMEM((n_fs, width, span), bf),
            pltpu.VMEM((2, rows, width), fl),
            pltpu.VMEM((rows, width), bf),
            pltpu.VMEM((n_tp, rows, feat), bf),
            pltpu.VMEM((rows, feat), bf),
            pltpu.VMEM((rows, feat), bf),
            pltpu.VMEM((3, length, feat), bf),
            pltpu.VMEM((n_fs // 2, length, feat), bf),
            pltpu.VMEM((n_tp, length, LANES), fl),
            pltpu.VMEM((length, feat), bf),
            dma(n_fs + 1),
            dma(2),
            dma(6),
            dma(n_fs + 1),
            dma(n_fs + 1),
            dma(n_fs + 1),
            dma(4 * n_fs),
            dma(9),
            dma(8),
            dma(2 * n_fs + 1),
            dma(7),
            dma(n_fs + 1),
        ],
        compiler_params=pltpu.CompilerParams(
            collective_id=0, has_side_effects=True, vmem_limit_bytes=60 * 2**20
        ),
    )(
        tokens[0],
        lin_weight,
        glu_weight,
        conv_taps,
        conv_gain[None],
        conv_out_weight,
        mix_gain[None],
        ff_gate,
        ff_up,
        ff_down,
        out_gain.reshape(n_tp, 1, feat),
    )
    return result


def widths(units, n_fs):
    half = n_fs // 2
    blocks = units // LANES // 2
    most = -(-blocks // half)
    return most * LANES, (blocks - most * (half - 1)) * LANES


def on_device(*args):
    tokens, lin_weight, conv_out_weight, ff_gate = args[0], args[1], args[5], args[7]
    n_fs, n_tp, n_rep = (lax.axis_size(a) for a in ("fs", "tp", "rep"))
    seqs, length, feat = tokens.shape
    units = ff_gate.shape[1]
    width, narrow = widths(units, n_fs)
    fits = (
        n_rep == 2
        and n_tp == 2
        and n_fs == 8
        and seqs == 1
        and length % 16 == 0
        and args[3].shape[0] <= 33
        and lin_weight.shape[1] * 2 == n_fs * LANES
        and conv_out_weight.shape[1] == n_tp * LANES
        and feat % (2 * LANES) == 0
        and units % (2 * LANES) == 0
        and narrow == width - LANES > 0
        and lin_weight.shape[0] % 32 == 0
    )
    if fits:
        return by_kernel(*args)
    return by_collectives(*args)


def solution(mesh):
    mapped = jax.shard_map(
        on_device,
        mesh=mesh,
        in_specs=(
            P(("rep", "fs"), None, "tp"),
            P("fs", "tp"),
            P("fs", "tp"),
            P(None, "tp"),
            P("tp"),
            P("tp", "fs"),
            P(),
            P("fs", "tp"),
            P("fs", "tp"),
            P("tp", "fs"),
            P(),
        ),
        out_specs=P(("rep", "fs"), None, "tp"),
        check_vma=False,
    )
    return mapped
```

```python
import functools

import jax
import jax.numpy as jnp
from jax import lax
from jax.experimental import pallas as pl
from jax.experimental.pallas import tpu as pltpu
from jax.sharding import PartitionSpec as P

residual_scale = 2.0**0.25
epsilon = 1e-05


def normed(values):
    average = jnp.mean(values, axis=-1, keepdims=True)
    second = jnp.mean(values * values, axis=-1, keepdims=True)
    return (values - average) * lax.rsqrt(second - average * average + epsilon)


def interleave(left, right, parts):
    rows, width = left.shape
    pair = jnp.concatenate(
        (left.reshape(rows, parts, width // parts), right.reshape(rows, parts, width // parts)),
        axis=2,
    )
    return pair.reshape(rows, 2 * width)


def by_collectives(
    tokens,
    lin_weight,
    glu_weight,
    conv_taps,
    conv_gain,
    conv_out_weight,
    mix_gain,
    ff_gate,
    ff_up,
    ff_down,
    out_gain,
):
    n_fs, n_tp = lax.axis_size("fs"), lax.axis_size("tp")
    fs_index, tp_index = lax.axis_index("fs"), lax.axis_index("tp")
    seqs, length, feat = tokens.shape
    groups = n_fs * seqs
    rows = groups * length
    model = feat * n_tp
    conv_gain_all = lax.all_gather(conv_gain, "tp", axis=0, tiled=True)

    gathered = lax.all_gather(tokens, ("fs", "tp"), axis=0, tiled=False)
    all_tokens = (
        gathered.reshape(n_fs, n_tp, seqs, length, feat)
        .transpose(0, 2, 3, 1, 4)
        .reshape(rows, model)
    )
    glu_pair = lax.all_to_all(
        interleave(lin_weight, glu_weight, n_fs), "fs", split_axis=1, concat_axis=0, tiled=True
    )
    own_out = lax.all_to_all(conv_out_weight, "tp", split_axis=1, concat_axis=0, tiled=True)
    ff_pair = lax.all_to_all(
        interleave(ff_gate, ff_up, n_fs), "fs", split_axis=1, concat_axis=0, tiled=True
    )
    own_down = lax.all_to_all(ff_down, "fs", split_axis=0, concat_axis=1, tiled=True)

    chans = glu_pair.shape[1] // 2
    product = jnp.dot(all_tokens, glu_pair, preferred_element_type=jnp.float32)
    glu = (product[:, :chans] * jax.nn.sigmoid(product[:, chans:])).astype(jnp.bfloat16)
    n_taps = conv_taps.shape[0]
    margin = (n_taps - 1) // 2
    own_taps = lax.dynamic_slice_in_dim(conv_taps, fs_index * chans, chans, 1)
    padded = jnp.pad(
        glu.astype(jnp.float32).reshape(groups, length, chans),
        ((0, 0), (margin, margin), (0, 0)),
    )
    conv = sum(padded[:, k : k + length] * own_taps[k] for k in range(n_taps))
    conv = conv.reshape(rows, chans).astype(jnp.bfloat16)
    conv_all = lax.all_gather(conv, ("tp", "fs"), axis=1, tiled=True)
    activated = jax.nn.silu(normed(conv_all.astype(jnp.float32)) * conv_gain_all).astype(
        jnp.bfloat16
    )
    mixed_own = jnp.dot(activated, own_out, preferred_element_type=jnp.float32).astype(
        jnp.bfloat16
    )
    mixed = lax.all_gather(mixed_own, ("fs", "tp"), axis=1, tiled=True)
    before = residual_scale * all_tokens.astype(jnp.float32) + mixed.astype(jnp.float32)
    middle = (normed(before) * mix_gain).astype(jnp.bfloat16)

    units = ff_pair.shape[1] // 2
    both = jnp.dot(middle, ff_pair, preferred_element_type=jnp.float32)
    hidden = (jax.nn.silu(both[:, :units]) * both[:, units:]).astype(jnp.bfloat16)
    down = jnp.dot(hidden, own_down, preferred_element_type=jnp.float32).astype(jnp.bfloat16)
    sends = (
        down.reshape(n_fs, seqs * length, n_tp, feat)
        .transpose(0, 2, 1, 3)
        .reshape(n_fs * n_tp, seqs * length, feat)
    )
    arrived = lax.all_to_all(sends, ("fs", "tp"), split_axis=0, concat_axis=0, tiled=True)
    forward = jnp.sum(arrived.astype(jnp.float32), axis=0)
    forward = forward.astype(jnp.bfloat16).astype(jnp.float32)
    middle_own = lax.dynamic_slice(
        middle,
        (fs_index * seqs * length, tp_index * feat),
        (seqs * length, feat),
    )
    final = residual_scale * middle_own.astype(jnp.float32) + forward
    sums, squares = lax.psum(
        (jnp.sum(final, axis=1, keepdims=True), jnp.sum(final * final, axis=1, keepdims=True)),
        "tp",
    )
    average = sums / model
    out = (final - average) * lax.rsqrt(squares / model - average * average + epsilon)
    gain = lax.dynamic_slice_in_dim(out_gain, tp_index * feat, feat, 0)
    return (out * gain).astype(jnp.bfloat16).reshape(seqs, length, feat)


MESH = pl.DeviceIdType.MESH
LANES = 128
FIRST = ((2, 0), (3, 0))
CROSS = ((2, 1), (3, 1))
NEAR = ((1, 0), (1, 1), (0, 1))
OTHERS = FIRST + CROSS + NEAR
G, U, D = 0, 1, 2
INNER = {
    "t0": ((1, G, 2, 0), (1, G, 3, 0), (1, G, 0, 1),),
    "t3": ((1, U, 2, 0),),
    "t5": ((1, U, 3, 0), (1, G, 1, 0),),
    "t6": ((1, G, 1, 1),),
    "t7": ((1, G, 2, 1), (1, D, 0, 1),),
    "c0": ((1, G, 3, 1),),
    "c2": ((0, G, 3, 0), (1, U, 1, 0),),
    "c3": ((1, U, 2, 1), (1, U, 3, 1),),
    "c4": ((0, G, 2, 0), (0, U, 3, 0), (1, U, 1, 1),),
    "c6": ((0, G, 1, 0), (0, U, 2, 0),),
    "c7": ((1, U, 0, 1), (1, D, 2, 0), (0, G, 0, 1),),
    "m0": ((1, D, 3, 0), (0, G, 3, 1), (0, G, 2, 1),),
    "m1": ((0, U, 3, 1), (0, U, 2, 1),),
    "m2": ((0, U, 1, 0), (0, U, 0, 1),),
    "m3": ((0, G, 1, 1),),
    "m4": ((1, D, 1, 0), (0, U, 1, 1),),
    "m5": ((1, D, 2, 1), (1, D, 3, 1), (1, D, 1, 1),),
    "m7": ((0, D, 2, 0),),
    "w2": ((0, D, 3, 1), (0, D, 2, 1),),
    "m8": ((0, D, 3, 0),),
}
OUTER = {
    "t3": ((1, G, 2, 0), (1, G, 3, 0),),
    "t5": ((1, U, 2, 0), (1, G, 1, 0),),
    "t7": ((1, D, 0, 1),),
    "c0": ((1, U, 3, 0),),
    "c2": ((0, G, 2, 0),),
    "c3": ((1, G, 2, 1), (1, G, 3, 1),),
    "c4": ((0, U, 2, 0), (0, G, 3, 0), (0, G, 1, 0),),
    "c5": ((1, U, 2, 1), (1, U, 3, 1),),
    "c6": ((0, U, 3, 0), (0, G, 1, 1),),
    "c7": ((1, U, 0, 1), (1, U, 1, 0), (1, G, 1, 1), (0, G, 0, 1),),
    "m0": ((1, U, 1, 1), (0, G, 2, 1), (0, G, 3, 1),),
    "m1": ((0, U, 2, 1),),
    "m2": ((0, U, 3, 1),),
    "m3": ((1, D, 2, 0), (0, U, 1, 0), (0, U, 0, 1),),
    "m4": ((0, U, 1, 1),),
    "m5": ((1, D, 3, 0), (1, D, 2, 1), (1, D, 3, 1),),
    "m7": ((0, D, 2, 0), (1, D, 1, 0), (1, D, 1, 1),),
    "w2": ((0, D, 3, 1), (0, D, 2, 1),),
    "t0": ((1, G, 0, 1),),
    "e0": ((0, D, 3, 0),),
}

def fused(
    n_fs,
    n_tp,
    width,
    narrow,
    tok,
    lin_hbm,
    glu_hbm,
    taps_hbm,
    gain,
    out_weight,
    mix_gain,
    gate_hbm,
    up_hbm,
    down_hbm,
    out_gain,
    out,
    x_s,
    lin_s,
    gl_s,
    taps_s,
    mix_s,
    glu_s,
    gain_s,
    proj_s,
    pad_s,
    conv_s,
    norm_s,
    act_s,
    mixed_s,
    mid_s,
    gate_s,
    up_s,
    down_s,
    ff_s,
    hid_s,
    part_s,
    half_s,
    sum_s,
    z_s,
    y_s,
    stat_s,
    out_s,
    glu_sems,
    glu_cross_sems,
    small_sems,
    tok_sems,
    conv_sems,
    mixed_sems,
    ff_sems,
    cross_sems,
    local_sems,
    half_sems,
    z_sems,
    y_sems,
):
    rep, f, t = lax.axis_index("rep"), lax.axis_index("fs"), lax.axis_index("tp")
    other = 1 - t
    n_hi = n_fs // 2
    hi, lo = f // 2, f % 2
    rows, feat = x_s.shape[1:]
    length = rows // n_fs
    model = feat * n_tp
    depth = gate_hbm.shape[0]
    half_depth = depth // 2
    chans = LANES // 2

    def flip(z, step):
        return z + step - 2 * step * ((z // step) % 2)

    def along(k):
        z = hi
        for step in (1, 2):
            if k[0] & step:
                z = flip(z, step)
        return z * 2 + (1 - lo if k[1] else lo)

    def code(k):
        return k[0] * 2 + k[1]

    barrier = pltpu.get_barrier_semaphore()
    for k in OTHERS:
        pl.semaphore_signal(barrier, inc=1, device_id=(rep, along(k), t), device_id_type=MESH)
    pl.semaphore_signal(barrier, inc=1, device_id=(rep, f, other), device_id_type=MESH)
    pl.semaphore_signal(barrier, inc=1, device_id=(1 - rep, f, t), device_id_type=MESH)

    def rows_of(i):
        return pl.ds(pl.multiple_of(i * length, length), length)

    def depth_of(i, part, size):
        return pl.ds(pl.multiple_of(i * depth + part * half_depth, half_depth), size)

    def tok_slot(i, j):
        return x_s.at[j, rows_of(i)]

    per_half = n_fs // 2

    def start_of(i):
        return pl.multiple_of((i * (width // LANES) - i // per_half) * LANES, LANES)

    def is_short(i):
        return i % per_half == per_half - 1

    def sized(i, action):
        @pl.when(jnp.logical_not(is_short(i)))
        def _():
            action(width)

        @pl.when(is_short(i))
        def _():
            action(narrow)

    fetches = [
        pltpu.make_async_copy(src, dst, local_sems.at[n])
        for n, (src, dst) in enumerate(
            (
                (tok, tok_slot(f, t)),
                (lin_hbm, lin_s),
                (glu_hbm, gl_s),
                (taps_hbm, taps_s),
            )
        )
    ]
    for copy in fetches:
        copy.start()

    def own_copy(which, size):
        first = start_of(f)
        src, dst = (
            (gate_hbm.at[:, pl.ds(first, size)], gate_s.at[depth_of(f, 0, depth), pl.ds(0, size)]),
            (up_hbm.at[:, pl.ds(first, size)], up_s.at[depth_of(f, 0, depth), pl.ds(0, size)]),
            (down_hbm.at[pl.ds(first, size)], down_s.at[f, pl.ds(0, size)]),
        )[which]
        return pltpu.make_async_copy(src, dst, local_sems.at[4 + which])

    for which in range(3):
        sized(f, lambda size, which=which: own_copy(which, size).start())

    @pl.when(is_short(f))
    def _():
        gate_s[:, narrow:] = jnp.zeros((n_fs * depth, width - narrow), jnp.bfloat16)
        up_s[:, narrow:] = jnp.zeros((n_fs * depth, width - narrow), jnp.bfloat16)
        down_s[:, narrow:, :] = jnp.zeros((n_fs, width - narrow, down_s.shape[2]), jnp.bfloat16)

    def remote(src, dst, send_sem, recv_sem, device):
        return pltpu.make_async_remote_copy(
            src_ref=src,
            dst_ref=dst,
            send_sem=send_sem,
            recv_sem=recv_sem,
            device_id=device,
            device_id_type=MESH,
        )

    def send(src, dst, sems, index, device):
        remote(src, dst, sems.at[0], sems.at[1 + index], device).start()

    partner = (rep, f, other)
    mirror = (1 - rep, f, t)
    beside = (rep, along((0, 1)), t)
    close = (rep, along((1, 0)), t)
    far = (rep, along((2, 0)), t)

    def arrive(dst, sem):
        remote(dst, dst, sem, sem, partner).wait_recv()

    def receive(dst, sems, index):
        arrive(dst, sems.at[1 + index])

    def sent(src, sem):
        remote(src, src, sem, sem, partner).wait_send()

    def small_copy(src, dst, index):
        return remote(src, dst, small_sems.at[index], small_sems.at[3 + index], partner)

    def gather_start(slot, sems):
        block = slot(f, t)
        send(block, block, sems, 0, far)
        send(block, block, sems, 1, close)
        send(block, block, sems, 3, beside)
        send(block, block, sems, 7, partner)

    inner = (hi % n_hi) // (n_hi // 2) != hi % 2

    def slot(name):
        for role, table in ((inner, INNER), (jnp.logical_not(inner), OUTER)):
            steps = table.get(name, ())

            @pl.when(role)
            def _(steps=steps):
                for send_it, which, *k in steps:
                    (weight_send if send_it else weight_forward)(which, tuple(k))

    def gather_finish(place, all_of, sems, name, between=None):
        between = between or {}

        def pause(step):
            slot(name + str(step))
            if step in between:
                between[step]()

        def got(index, k):
            block = place(along(k), t)
            receive(block, sems, index)
            return block

        block = got(3, (0, 1))
        send(block, block, sems, 7, partner)
        pause(1)
        block = got(0, (2, 0))
        send(block, block, sems, 2, close)
        send(block, block, sems, 5, beside)
        send(block, block, sems, 7, partner)
        pause(2)
        block = got(1, (1, 0))
        send(block, block, sems, 4, beside)
        send(block, block, sems, 7, partner)
        pause(3)
        block = got(4, (1, 1))
        send(block, block, sems, 7, partner)
        pause(4)
        block = got(2, (3, 0))
        send(block, block, sems, 6, beside)
        send(block, block, sems, 7, partner)
        pause(5)
        block = got(5, (2, 1))
        send(block, block, sems, 7, partner)
        pause(6)
        block = got(6, (3, 1))
        send(block, block, sems, 7, partner)
        pause(7)
        receive(all_of(other), sems, 7)

    half_width = width // 2

    def piece(which, to, source, part, size):
        first = start_of(to)
        ups = pl.ds(pl.multiple_of(part * half_depth, half_depth), half_depth)
        spot = depth_of(source, part, half_depth)
        deep = pl.ds(pl.multiple_of(part * (size // 2), size // 2), size // 2)
        from_down = pl.ds(pl.multiple_of(first + part * (size // 2), LANES // 2), size // 2)
        return (
            (gate_hbm.at[ups, pl.ds(first, size)], gate_s.at[spot, pl.ds(0, size)]),
            (up_hbm.at[ups, pl.ds(first, size)], up_s.at[spot, pl.ds(0, size)]),
            (down_hbm.at[from_down], down_s.at[source, deep]),
        )[which]

    def whole(which, k):
        return which == D and k in NEAR

    def weight_copy(which, k, size):
        to = along(k)
        if whole(which, k):
            src, dst = down_hbm.at[pl.ds(start_of(to), size)], down_s.at[f, pl.ds(0, size)]
        else:
            src, dst = piece(which, to, f, rep, size)
        return remote(
            src, dst, ff_sems.at[3 * n_fs + code(k)], ff_sems.at[which * n_fs + code(k)], (rep, to, t)
        )

    def weight_send(which, k):
        sized(along(k), lambda size: weight_copy(which, k, size).start())

    def group_sem(which, k):
        group = 0 if k in NEAR else 1 if k in FIRST else 2
        return cross_sems.at[2 + (6 if which == D else 3 * which + group)]

    def cross_copy(which, k, size):
        block = piece(which, f, along(k), rep, size)[1]
        return remote(block, block, cross_sems.at[which // 2], group_sem(which, k), mirror)

    def weight_forward(which, k):
        def action(size):
            block = piece(which, f, along(k), rep, size)[1]
            arrive(block, ff_sems.at[which * n_fs + code(k)])
            cross_copy(which, k, size).start()

        sized(f, action)

    def weight_finish(which, ks):
        def action(size):
            if whole(which, ks[0]):
                for k in ks:
                    arrive(down_s.at[along(k), pl.ds(0, size)], ff_sems.at[which * n_fs + code(k)])
            else:
                arrive(
                    gate_s.at[pl.ds(0, len(ks) * half_depth), pl.ds(0, size)],
                    group_sem(which, ks[0]),
                )

        sized(f, action)

    pl.semaphore_wait(barrier, n_fs + 1)
    fetches[0].wait()
    gather_start(tok_slot, tok_sems)
    fetches[1].wait()
    fetches[2].wait()
    for d in range(n_fs):
        cols = slice(d * chans, (d + 1) * chans)
        mix_s[d] = jnp.concatenate((lin_s[:, cols], gl_s[:, cols]), axis=1)

    def glu_piece(source, part):
        return glu_s.at[depth_of(source, part, half_depth)]

    for k in OTHERS:
        to = along(k)
        own_rows = pl.ds(pl.multiple_of(rep * half_depth, half_depth), half_depth)
        send(mix_s.at[to, own_rows], glu_piece(f, rep), glu_sems, code(k), (rep, to, t))
    slot("t0")
    columns = pl.ds(pl.multiple_of(other * LANES, LANES), LANES)
    own_columns = pl.ds(pl.multiple_of(t * LANES, LANES), LANES)
    small_copy(gain, gain_s.at[t], 0).start()
    small_copy(out_weight.at[:, columns], proj_s.at[t], 1).start()

    glu_s[pl.ds(pl.multiple_of(f * depth, depth), depth), :] = mix_s[f]
    gain_s[t] = gain[...]
    proj_s[t] = out_weight[:, own_columns]
    pad_s[...] = jnp.zeros_like(pad_s)

    def glu_forward(ks):
        for k in ks:
            block = glu_piece(along(k), rep)
            receive(block, glu_sems, code(k))
            send(block, block, glu_cross_sems, 0, mirror)

    gather_finish(
        tok_slot,
        lambda j: x_s.at[j],
        tok_sems,
        "t",
        {
            4: lambda: glu_forward(NEAR),
            5: lambda: glu_forward(FIRST),
            6: lambda: glu_forward(CROSS),
        },
    )
    seven = glu_s.at[pl.ds(0, len(OTHERS) * half_depth)]
    receive(seven, glu_cross_sems, 0)

    product = sum(
        jnp.dot(
            x_s[j], glu_s[j * feat : (j + 1) * feat], preferred_element_type=jnp.float32
        )
        for j in range(n_tp)
    )
    glu = product[:, :chans] / (1.0 + jnp.exp(-product[:, chans:]))
    top = rows // 2
    packed = jnp.concatenate((glu[:top], glu[top:]), axis=1)
    packed = packed.astype(jnp.bfloat16).astype(jnp.float32)
    fetches[3].wait()
    lanes = lax.broadcasted_iota(jnp.int32, (1, LANES), 1)
    tap_pair = taps_s[:, pl.ds(pl.multiple_of(f // 2 * LANES, LANES), LANES)]
    turned = pltpu.roll(tap_pair, chans, 1)
    taps = jnp.where((lanes < chans) == (f % 2 == 0), tap_pair, turned)
    n_taps = taps.shape[0]
    margin = (n_taps - 1) // 2
    slot("d0")
    conv_slot = lambda i, j: conv_s.at[j * n_fs + i]
    groups = n_fs // 2
    for g in range(groups):
        pad_s[g, 16 : 16 + length, :] = packed[g * length : (g + 1) * length]
    for g in range(groups):
        acc = jnp.zeros((length, LANES), jnp.float32)
        for k in range(n_taps):
            first = 16 - margin + k
            acc = acc + pad_s[g, first : first + length, :] * taps[k : k + 1, :]
        conv_s[t * n_fs + f, g * length : (g + 1) * length, :] = acc.astype(jnp.bfloat16)
    gather_start(conv_slot, conv_sems)
    slot("c0")
    gather_finish(
        conv_slot, lambda j: conv_s.at[pl.ds(j * n_fs, n_fs)], conv_sems, "c"
    )
    small_copy(gain_s.at[other], gain_s.at[other], 0).wait_recv()
    small_copy(proj_s.at[other], proj_s.at[other], 1).wait_recv()

    for j in range(n_fs * n_tp // 2):
        left = conv_s[2 * j].astype(jnp.float32)
        right = conv_s[2 * j + 1].astype(jnp.float32)
        cols = slice(j * LANES, (j + 1) * LANES)
        norm_s[:top, cols] = jnp.concatenate((left[:, :chans], right[:, :chans]), axis=1)
        norm_s[top:, cols] = jnp.concatenate((left[:, chans:], right[:, chans:]), axis=1)
    gains = jnp.concatenate([gain_s[j] for j in range(n_tp)], axis=1)

    @pl.loop(0, n_fs)
    def _(i):
        here = rows_of(i)
        v = normed(norm_s[here, :]) * gains
        act_s[here, :] = (v / (1.0 + jnp.exp(-v))).astype(jnp.bfloat16)

    slot("n0")
    share = proj_s.shape[1]
    mixed_slot = lambda i, j: mixed_s.at[j * n_fs + i]
    mixed_s[t * n_fs + f] = sum(
        jnp.dot(
            act_s[:, j * share : (j + 1) * share],
            proj_s[j],
            preferred_element_type=jnp.float32,
        )
        for j in range(n_tp)
    ).astype(jnp.bfloat16)
    gather_start(mixed_slot, mixed_sems)
    slot("m0")
    gather_finish(
        mixed_slot, lambda j: mixed_s.at[pl.ds(j * n_fs, n_fs)], mixed_sems, "m"
    )
    slot("m8")

    @pl.loop(0, n_fs)
    def _(i):
        here = rows_of(i)
        skip = jnp.concatenate([x_s[j, here, :] for j in range(n_tp)], axis=1)
        added = jnp.concatenate(
            [mixed_s[j * n_fs + k, here, :] for k in range(n_fs) for j in range(n_tp)], axis=1
        )
        before = residual_scale * skip.astype(jnp.float32) + added.astype(jnp.float32)
        mid_s[here, :] = (normed(before) * mix_gain[...]).astype(jnp.bfloat16)

    slot("e0")
    near_side = hi // (n_hi // 2)
    deep = n_fs // n_tp * depth

    def partial_ff(side):
        inner_rows = pl.ds(pl.multiple_of(side * deep, deep), deep)
        left = mid_s[:, inner_rows]
        return tuple(
            jnp.dot(left, right[inner_rows, :], preferred_element_type=jnp.float32)
            for right in (gate_s, up_s)
        )

    for which in (0, 1):
        sized(f, lambda size: own_copy(which, size).wait())
        weight_finish(which, NEAR)
        slot("w" + str(which))
    ff_s[0], ff_s[1] = partial_ff(near_side)
    slot("w2")
    for i, (which, ks) in enumerate(((0, FIRST), (1, FIRST), (0, CROSS), (1, CROSS))):
        weight_finish(which, ks)
        slot("w" + str(3 + i))

    gate, upward = partial_ff(1 - near_side)
    gate, upward = gate + ff_s[0], upward + ff_s[1]
    hid_s[...] = (gate / (1.0 + jnp.exp(-gate)) * upward).astype(jnp.bfloat16)
    slot("g0")

    sized(f, lambda size: own_copy(2, size).wait())
    weight_finish(2, NEAR)
    slot("g2")
    span = down_s.shape[2]
    per_core = n_fs // n_tp
    steps = (3, 2, 1, 0)

    def project(side):
        @pl.loop(0, per_core)
        def _(j):
            part_s[side, :, pl.ds(pl.multiple_of(j * span, span), span)] = jnp.dot(
                hid_s[...], down_s[side * per_core + j], preferred_element_type=jnp.float32
            ).astype(jnp.bfloat16)

    pieces_of = tuple((d, h) for d in steps for h in (0, 1))

    def cols(h):
        return pl.ds(h * (feat // 2), feat // 2)

    def half_copy(k, h):
        here = rows_of(along(k))
        return remote(
            part_s.at[other, here, cols(h)],
            half_s.at[here, cols(h)],
            half_sems.at[0],
            half_sems.at[1 + 2 * code(k) + h],
            partner,
        )

    def hand_over():
        for low in (1, 0):
            for d, h in pieces_of:
                half_copy((d, low), h).start()

    def joined(k, h):
        here = rows_of(along(k))
        receive(half_s.at[here, cols(h)], half_sems, 2 * code(k) + h)
        return part_s[t, here, cols(h)].astype(jnp.float32) + half_s[here, cols(h)].astype(
            jnp.float32
        )

    def aside_copy(d, h):
        return remote(
            sum_s.at[rows_of(along((d, 1))), cols(h)],
            y_s.at[d, :, cols(h)],
            y_sems.at[0],
            y_sems.at[1 + 2 * d + h],
            beside,
        )

    def aside():
        for d, h in pieces_of:
            sum_s[rows_of(along((d, 1))), cols(h)] = joined((d, 1), h).astype(jnp.bfloat16)
            aside_copy(d, h).start()

    project(near_side)
    pl.when(t == near_side)(aside)
    pl.when(t != near_side)(hand_over)
    slot("g3")
    weight_finish(2, FIRST + CROSS)
    project(1 - near_side)
    pl.when(t == near_side)(hand_over)
    pl.when(t != near_side)(aside)

    def z_part(i, h):
        return z_s.at[i, :, cols(h)]

    ends = []
    for d, h in pieces_of:
        here = rows_of(along((d, 0)))
        forward = joined((d, 0), h)
        receive(y_s.at[d, :, cols(h)], y_sems, 2 * d + h)
        forward = forward + y_s[d, :, cols(h)].astype(jnp.float32)
        if d == 2:
            receive(z_part(1, h), z_sems, 2 + h)
            forward = forward + z_s[1, :, cols(h)].astype(jnp.float32)
        if d:
            sum_s[here, cols(h)] = forward.astype(jnp.bfloat16)
            slot_of = d // 2 if d % 2 else 2
            send(
                sum_s.at[here, cols(h)],
                z_part(slot_of, h),
                z_sems,
                2 * slot_of + h,
                close if d % 2 else far,
            )
        else:
            ends.append(forward)
    for i in (0, 2):
        for h in (0, 1):
            receive(z_part(i, h), z_sems, 2 * i + h)
            ends[h] = ends[h] + z_s[i, :, cols(h)].astype(jnp.float32)
    forward = jnp.concatenate(ends, axis=1)
    forward = forward.astype(jnp.bfloat16).astype(jnp.float32)
    own_half = pl.ds(pl.multiple_of(t * feat, feat), feat)
    final = residual_scale * mid_s[rows_of(f), own_half].astype(jnp.float32) + forward
    lane = lax.broadcasted_iota(jnp.int32, (length, LANES), 1)
    stat_s[t] = jnp.where(
        lane == 0,
        jnp.sum(final, axis=1, keepdims=True),
        jnp.sum(final * final, axis=1, keepdims=True),
    )
    small_copy(stat_s.at[t], stat_s.at[t], 2).start()
    small_copy(stat_s.at[other], stat_s.at[other], 2).wait_recv()
    stats = (stat_s[0] + stat_s[1]) / model
    average, second = stats[:, 0:1], stats[:, 1:2]
    scaled = (final - average) * lax.rsqrt(second - average * average + epsilon)
    out_s[...] = (scaled * out_gain[t]).astype(jnp.bfloat16)
    result = pltpu.make_async_copy(out_s, out.at[0], local_sems.at[7])
    result.start()
    result.wait()
    blocks = n_fs * n_tp - 1
    sent(mixed_s.at[pl.ds(0, blocks)], tok_sems.at[0])
    sent(conv_s.at[pl.ds(0, blocks)], conv_sems.at[0])
    sent(mixed_s.at[pl.ds(0, blocks)], mixed_sems.at[0])
    sent(seven, glu_sems.at[0])
    sent(seven, glu_cross_sems.at[0])
    sent(half_s, half_sems.at[0])
    sent(y_s, y_sems.at[0])
    sent(z_s, z_sems.at[0])
    small_copy(gain, gain_s.at[t], 0).wait_send()
    small_copy(out_weight.at[:, columns], proj_s.at[t], 1).wait_send()
    small_copy(stat_s.at[t], stat_s.at[t], 2).wait_send()
    for k in OTHERS:
        deep_rows = pl.ds(0, (4 if k in NEAR else 3) * half_depth)
        sized(
            along(k),
            lambda size: sent(
                gate_s.at[deep_rows, pl.ds(0, size)], ff_sems.at[3 * n_fs + code(k)]
            ),
        )
    for i, count in enumerate((2 * len(OTHERS), len(FIRST + CROSS))):
        sized(
            f,
            lambda size: sent(
                gate_s.at[pl.ds(0, count * half_depth), pl.ds(0, size)], cross_sems.at[i]
            ),
        )


def by_kernel(
    tokens,
    lin_weight,
    glu_weight,
    conv_taps,
    conv_gain,
    conv_out_weight,
    mix_gain,
    ff_gate,
    ff_up,
    ff_down,
    out_gain,
):
    n_fs, n_tp = lax.axis_size("fs"), lax.axis_size("tp")
    _, length, feat = tokens.shape
    rows, model = n_fs * length, feat * n_tp
    depth, own_chans = lin_weight.shape
    chans = own_chans // n_fs
    width, narrow = widths(ff_gate.shape[1], n_fs)
    vmem, far = pl.BlockSpec(memory_space=pltpu.VMEM), pl.BlockSpec(memory_space=pl.ANY)
    bf, fl = jnp.bfloat16, jnp.float32
    span = ff_down.shape[1]
    dma = lambda n: pltpu.SemaphoreType.DMA((n,))
    result = pl.pallas_call(
        functools.partial(fused, n_fs, n_tp, width, narrow),
        out_shape=jax.ShapeDtypeStruct((1, length, feat), bf),
        in_specs=[far] * 4 + [vmem] * 3 + [far] * 3 + [vmem],
        out_specs=far,
        scratch_shapes=[
            pltpu.VMEM((n_tp, rows, feat), bf),
            pltpu.VMEM((depth, own_chans), bf),
            pltpu.VMEM((depth, own_chans), bf),
            pltpu.VMEM(conv_taps.shape, fl),
            pltpu.VMEM((n_fs, depth, 2 * chans), bf),
            pltpu.VMEM((n_fs * depth, 2 * chans), bf),
            pltpu.VMEM((n_tp, 1, own_chans), fl),
            pltpu.VMEM((n_tp, own_chans, span // n_tp), bf),
            pltpu.VMEM((n_fs // 2, length + 32, LANES), fl),
            pltpu.VMEM((n_fs * n_tp, rows // 2, LANES), bf),
            pltpu.VMEM((rows, own_chans * n_tp), fl),
            pltpu.VMEM((rows, own_chans * n_tp), bf),
            pltpu.VMEM((n_fs * n_tp, rows, LANES), bf),
            pltpu.VMEM((rows, model), bf),
            pltpu.VMEM((n_fs * depth, width), bf),
            pltpu.VMEM((n_fs * depth, width), bf),
            pltpu.VMEM((n_fs, width, span), bf),
            pltpu.VMEM((2, rows, width), fl),
            pltpu.VMEM((rows, width), bf),
            pltpu.VMEM((n_tp, rows, feat), bf),
            pltpu.VMEM((rows, feat), bf),
            pltpu.VMEM((rows, feat), bf),
            pltpu.VMEM((3, length, feat), bf),
            pltpu.VMEM((n_fs // 2, length, feat), bf),
            pltpu.VMEM((n_tp, length, LANES), fl),
            pltpu.VMEM((length, feat), bf),
            dma(n_fs + 1),
            dma(2),
            dma(6),
            dma(n_fs + 1),
            dma(n_fs + 1),
            dma(n_fs + 1),
            dma(4 * n_fs),
            dma(9),
            dma(8),
            dma(2 * n_fs + 1),
            dma(7),
            dma(n_fs + 1),
        ],
        compiler_params=pltpu.CompilerParams(
            collective_id=0, has_side_effects=True, vmem_limit_bytes=60 * 2**20
        ),
    )(
        tokens[0],
        lin_weight,
        glu_weight,
        conv_taps,
        conv_gain[None],
        conv_out_weight,
        mix_gain[None],
        ff_gate,
        ff_up,
        ff_down,
        out_gain.reshape(n_tp, 1, feat),
    )
    return result


def widths(units, n_fs):
    half = n_fs // 2
    blocks = units // LANES // 2
    most = -(-blocks // half)
    return most * LANES, (blocks - most * (half - 1)) * LANES


def on_device(*args):
    tokens, lin_weight, conv_out_weight, ff_gate = args[0], args[1], args[5], args[7]
    n_fs, n_tp, n_rep = (lax.axis_size(a) for a in ("fs", "tp", "rep"))
    seqs, length, feat = tokens.shape
    units = ff_gate.shape[1]
    width, narrow = widths(units, n_fs)
    fits = (
        n_rep == 2
        and n_tp == 2
        and n_fs == 8
        and seqs == 1
        and length % 16 == 0
        and args[3].shape[0] <= 33
        and lin_weight.shape[1] * 2 == n_fs * LANES
        and conv_out_weight.shape[1] == n_tp * LANES
        and feat % (2 * LANES) == 0
        and units % (2 * LANES) == 0
        and narrow == width - LANES > 0
        and lin_weight.shape[0] % 32 == 0
    )
    if fits:
        return by_kernel(*args)
    return by_collectives(*args)


def solution(mesh):
    mapped = jax.shard_map(
        on_device,
        mesh=mesh,
        in_specs=(
            P(("rep", "fs"), None, "tp"),
            P("fs", "tp"),
            P("fs", "tp"),
            P(None, "tp"),
            P("tp"),
            P("tp", "fs"),
            P(),
            P("fs", "tp"),
            P("fs", "tp"),
            P("tp", "fs"),
            P(),
        ),
        out_specs=P(("rep", "fs"), None, "tp"),
        check_vma=False,
    )
    return mapped
```
